256 devices in a mesh: fs: 32 (over z, y), tp: 8 (over x, core).
Axes of the slice: x: 4, y: 4, z: 8, core: 2. Of those that a mesh axis runs over, the one named last changes fastest.
Arguments:
- tokens: bfloat16 [65536, 2048], P(('fs', 'tp')), may hold values from -6 to 6
- expert_group: int32 [65536], P(('fs', 'tp')), may hold values from 0 to 7, as said below
- expert_fine: int32 [65536, 2], P(('fs', 'tp')), may hold values from 0 to 3, as said below
- route_weight: float32 [65536, 2], P(('fs', 'tp')), may hold values from 0.2 to 0.9
- norm_gain: float32 [2048], P('fs'), may hold values from 0.1 to 1.9
- gate_master: float32 [32, 2048, 512], P(None, 'fs', 'tp'), may hold values from -0.125 to 0.125
- up_master: float32 [32, 2048, 512], P(None, 'fs', 'tp'), may hold values from -0.125 to 0.125
- down_master: float32 [32, 2048, 512], P(None, 'fs', 'tp'), may hold values from -0.25 to 0.25
Outputs:
- mixed: bfloat16 [65536, 2048], P(('fs', 'tp'))
- gate_ready: bfloat16 [32, 2048, 512], P('fs')
- up_ready: bfloat16 [32, 2048, 512], P('fs')
- down_ready: bfloat16 [32, 2048, 512], P('fs')
The draws below stay inside these ranges and needn't reach their ends.
Inputs may be any that keep to these rules, and one draw needn't show every extreme that they name: `expert_group`: in the rows of one device every group is chosen by the same number of rows. `expert_fine`: the two entries of a row differ. Counting an expert as its group and entry, the rows of one device name one expert at most 32 times, and in every group one expert is named exactly 32 times by the rows of every device.
All inputs are finite; a program needn't handle non-finite values.
Results may differ from the reference program's by a relative error of at most 0.0086.
Values may be sent and summed in bfloat16 or wider, within the bound.
A program may use at most 128 MiB of HBM per device.

```python
import jax
import jax.numpy as jnp
from jax import lax

D = 2048
F = 512
FINE = 4
TOP = 2
TOK_DEV = 256
EXPERTS = 32
GROUPS = 8
CAP = 32
TOKENS = 65536
DEVICES = 256


def route_tables(key):
    base = jax.random.fold_in(key, 7)
    blocks = TOKENS // TOK_DEV
    per_group = TOK_DEV // GROUPS
    pattern = jnp.array([16, 8, 5, 3], jnp.int32)
    hot_key = jax.random.fold_in(base, 1)
    perm_key = jax.random.fold_in(base, 2)
    shuffle_key = jax.random.fold_in(base, 3)
    hot = jax.random.randint(hot_key, (GROUPS,), 0, FINE)
    perms = jax.vmap(lambda sub: jax.random.permutation(sub, FINE))(jax.random.split(perm_key, blocks * GROUPS))
    perms = perms.reshape(blocks, GROUPS, FINE).astype(jnp.int32)
    raw = pattern[perms]
    column = jnp.arange(FINE, dtype=jnp.int32)
    top_pos = jnp.sum(column * (perms == 0).astype(jnp.int32), axis=-1)
    is_hot = column[None, None, :] == hot[None, :, None]
    raw_hot = jnp.sum(raw * is_hot.astype(jnp.int32), axis=-1, keepdims=True)
    weight = jnp.where(is_hot, 16, jnp.where(column[None, None, :] == top_pos[..., None], raw_hot, raw))
    counts = weight * CAP // 16
    bounds = jnp.cumsum(counts, axis=-1)
    within = jnp.arange(per_group, dtype=jnp.int32)
    first = jnp.sum((within[None, None, :, None] >= bounds[:, :, None, :]).astype(jnp.int32), axis=-1)
    second = jnp.sum(((within + per_group)[None, None, :, None] >= bounds[:, :, None, :]).astype(jnp.int32), axis=-1)
    group = jnp.broadcast_to(jnp.arange(GROUPS, dtype=jnp.int32)[None, :, None], first.shape)
    group = group.reshape(blocks, TOK_DEV)
    fine = jnp.stack([first, second], axis=-1).reshape(blocks, TOK_DEV, 2)
    shuffle = jax.vmap(lambda sub: jax.random.permutation(sub, TOK_DEV))(jax.random.split(shuffle_key, blocks)).astype(jnp.int32)
    group = jnp.take_along_axis(group, shuffle, axis=1)
    fine = jnp.take_along_axis(fine, shuffle[:, :, None], axis=1)
    return (group.reshape(TOKENS).astype(jnp.int32), fine.reshape(TOKENS, 2).astype(jnp.int32))


def draw_expert_group(key, part):
    return route_tables(key)[0]


def draw_expert_fine(key, part):
    return route_tables(key)[1]


def shard_levels(stream_key, extent, cuts, low, largest):
    loudness = 1.0
    for dim, parts in cuts:
        steps = jax.random.uniform(jax.random.fold_in(jax.random.fold_in(stream_key, 6), dim), (parts,), jnp.float32, low / len(cuts), largest / len(cuts))
        loudness = loudness * jnp.repeat(jnp.exp(steps), extent[dim] // parts).reshape((-1,) + (1,) * (len(extent) - 1 - dim))
    return loudness


def noise(rng, dims, deviation, most, cuts=(), held_as=jnp.bfloat16):
    loudness = shard_levels(rng, dims, cuts, -0.22, 0.18) if cuts else 1.0
    values = jax.random.normal(rng, dims, jnp.float32) * deviation * loudness
    return jnp.minimum(jnp.maximum(values, -most), most).astype(held_as)


def setup_inputs(seed: int = 0) -> dict:
    key_of = jax.random.split(jax.random.key(seed), 9)
    return {
        "tokens": noise(key_of[0], (TOKENS, D), 1.0, 6.0, ((0, 256),)),
        "expert_group": draw_expert_group(jax.random.fold_in(key_of[8], 71), 0),
        "expert_fine": draw_expert_fine(jax.random.fold_in(key_of[8], 71), 0),
        "route_weight": jnp.clip(0.2 + 0.7 * jax.random.uniform(key_of[3], (TOKENS, TOP), jnp.float32) ** shard_levels(key_of[3], (TOKENS, TOP), ((0, 256),), -0.2, 0.2), 0.2, 0.9),
        "norm_gain": jnp.clip(1.0 + 0.18 * jax.random.normal(key_of[4], (D,), jnp.float32), 0.1, 1.9),
        "gate_master": noise(key_of[5], (EXPERTS, D, F), D ** -0.5, 0.125, ((1, 32), (2, 8)), jnp.float32),
        "up_master": noise(key_of[6], (EXPERTS, D, F), D ** -0.5, 0.125, ((1, 32), (2, 8)), jnp.float32),
        "down_master": noise(key_of[7], (EXPERTS, D, F), F ** -0.5, 0.25, ((1, 32), (2, 8)), jnp.float32),
    }


EPS = 1e-06

def reference(tokens, expert_group, expert_fine, route_weight, norm_gain, gate_master, up_master, down_master):
    gate_ready = (norm_gain[None, :, None] * gate_master).astype(jnp.bfloat16)
    up_ready = (norm_gain[None, :, None] * up_master).astype(jnp.bfloat16)
    down_ready = down_master.astype(jnp.bfloat16)
    widened = tokens.astype(jnp.float32)
    normed = (widened * lax.rsqrt(lax.optimization_barrier(jnp.mean(widened * widened, axis=-1, keepdims=True)) + EPS)).astype(jnp.bfloat16)
    expert = (FINE * expert_group[:, None] + expert_fine).reshape(-1).astype(jnp.int32)
    weights = route_weight.reshape(-1)
    slot_count = DEVICES * CAP

    def per_expert(totals, expert_id):
        hits = expert == expert_id
        chosen = jnp.nonzero(hits, size=slot_count, fill_value=0)[0].astype(jnp.int32)
        filled = jnp.arange(slot_count, dtype=jnp.int32) < jnp.sum(hits.astype(jnp.int32))
        source_row = chosen // TOP
        input_rows = normed[source_row]
        gate_value = jnp.dot(input_rows, gate_ready[expert_id], preferred_element_type=jnp.float32)
        upward = jnp.dot(input_rows, up_ready[expert_id], preferred_element_type=jnp.float32)
        activation = (jax.nn.silu(gate_value) * upward).astype(jnp.bfloat16)
        produced = lax.dot_general(activation, down_ready[expert_id], (((1,), (1,)), ((), ())), preferred_element_type=jnp.float32).astype(jnp.bfloat16)
        scale = jnp.where(filled, weights[chosen], jnp.zeros((), weights.dtype)).astype(jnp.float32)
        totals = totals.at[source_row].add(scale[:, None] * produced.astype(jnp.float32))
        return (totals, None)
    totals, _ = lax.scan(per_expert, jnp.zeros((TOKENS, D), jnp.float32), jnp.arange(EXPERTS, dtype=jnp.int32))
    mixed = totals.astype(jnp.bfloat16)
    return (mixed, gate_ready, up_ready, down_ready)
```

```python
import jax
import jax.numpy as jnp
from jax import lax
from jax.sharding import Mesh, PartitionSpec as P

FINE = 4
EPS = 1e-06
BF = jnp.bfloat16


def exchange_weights(gate_piece, up_piece, down_piece):
    both = jnp.concatenate((gate_piece, up_piece, down_piece), axis=2)
    filled = lax.all_to_all(both, ("z", "y"), split_axis=0, concat_axis=1, tiled=True)
    parts = jnp.split(filled, 3, axis=2)
    return tuple(lax.all_gather(a, ("x", "c"), axis=2, tiled=True) for a in parts)


def local(
    tokens, expert_group, expert_fine, route_weight, norm_gain, gate_master, up_master, down_master
):
    gate_piece = (norm_gain[None, :, None] * gate_master).astype(BF)
    up_piece = (norm_gain[None, :, None] * up_master).astype(BF)
    down_piece = down_master.astype(BF)
    gate_ready, up_ready, down_ready = exchange_weights(gate_piece, up_piece, down_piece)

    rows, width = tokens.shape
    groups = lax.axis_size("z")
    per_group = rows // groups
    widened = tokens.astype(jnp.float32)
    normed = (
        widened * lax.rsqrt(jnp.mean(widened * widened, axis=-1, keepdims=True) + EPS)
    ).astype(BF)
    same = (expert_group[:, None] == jnp.arange(groups)[None, :]).astype(BF)
    ahead = jnp.arange(rows)[:, None] > jnp.arange(rows)[None, :]
    before = jnp.dot(ahead.astype(BF), same, preferred_element_type=jnp.float32)
    position = jnp.sum(before * same.astype(jnp.float32), axis=1).astype(jnp.int32)
    slot = expert_group * per_group + position
    placing = (jnp.arange(rows, dtype=jnp.int32)[:, None] == slot[None, :]).astype(BF)
    fine_weight = jnp.sum(
        jnp.where(
            expert_fine[:, :, None] == jnp.arange(FINE)[None, None, :],
            route_weight[:, :, None],
            0.0,
        ),
        axis=1,
    )
    high = fine_weight.astype(BF)
    rest = fine_weight - high.astype(jnp.float32)
    low = rest.astype(BF)
    packed = jnp.concatenate(
        (normed, high, low, jnp.zeros((rows, 128 - 2 * FINE), BF)), axis=1
    )
    outgoing = jnp.dot(placing, packed, preferred_element_type=jnp.float32).astype(BF)
    outgoing = outgoing.reshape(groups, per_group, width + 128)
    arrived = lax.all_to_all(outgoing, "z", split_axis=0, concat_axis=0, tiled=True)
    gathered = lax.all_gather(arrived, "y", axis=0, tiled=False)
    gathered = gathered.reshape(FINE * rows, width + 128)
    data = gathered[:, :width]
    mine = lax.axis_index("y")
    pick = (jnp.arange(FINE) == mine).astype(jnp.float32)[None, :]
    scale = jnp.sum(
        pick
        * (
            gathered[:, width : width + FINE].astype(jnp.float32)
            + gathered[:, width + FINE : width + 2 * FINE].astype(jnp.float32)
        ),
        axis=1,
        keepdims=True,
    )
    gate_value = jnp.dot(data, gate_ready[0], preferred_element_type=jnp.float32)
    upward = jnp.dot(data, up_ready[0], preferred_element_type=jnp.float32)
    activation = (jax.nn.silu(gate_value) * upward).astype(BF)
    out = lax.dot_general(
        activation, down_ready[0], (((1,), (1,)), ((), ())), preferred_element_type=jnp.float32
    )
    out = (out.astype(BF).astype(jnp.float32) * scale).astype(BF)
    summed = lax.psum_scatter(out, "y", scatter_dimension=0, tiled=True)
    back = lax.all_to_all(
        summed.reshape(groups, per_group, width), "z", split_axis=0, concat_axis=0, tiled=True
    )
    mixed = lax.dot_general(
        placing,
        back.reshape(rows, width),
        (((0,), (0,)), ((), ())),
        preferred_element_type=jnp.float32,
    ).astype(BF)
    return (mixed, gate_ready, up_ready, down_ready)


def solution(mesh):
    fine = Mesh(mesh.devices.reshape(8, 4, 4, 2), ("z", "y", "x", "c"))
    fs, tp = ("z", "y"), ("x", "c")
    token = fs + tp
    in_specs = (
        P(token, None),
        P(token),
        P(token, None),
        P(token, None),
        P(fs),
        P(None, fs, tp),
        P(None, fs, tp),
        P(None, fs, tp),
    )
    out_specs = (
        P(token, None),
        P(fs, None, None),
        P(fs, None, None),
        P(fs, None, None),
    )
    return jax.shard_map(local, mesh=fine, in_specs=in_specs, out_specs=out_specs, check_vma=False)
```

```python
import jax
import jax.numpy as jnp
from jax import lax
from jax.experimental import pallas as pl
from jax.experimental.pallas import tpu as pltpu
from jax.sharding import Mesh, PartitionSpec as P

FINE = 4
EPS = 1e-06
BF = jnp.bfloat16
F32 = jnp.float32
NZ, NY, NX = 8, 4, 4
ROWS = 32
HALF = 16
D = 2048
LANE = 128
WIDE = D + LANE
MESH = pl.DeviceIdType.MESH


def offset_of(s):
    far = (s + 1) // 2
    odd = s % 2
    return (odd * far + (1 - odd) * (NZ - far)) % NZ


def kernel(
    rows_in, pieces, back_out, gate_out, up_out, down_out,
    a, o, h, f, zsum, back, w, wsend, wz, other,
    zt_s, zt_r, zw_s, zw_r, ag_s, ag_r, yw_s, yw_r, xw_s, xw_r, cw_s, cw_r,
    pair_s, pair_r, rs_s, rs_r, zb_s, zb_r, out_sem, back_sem,
):
    z, y, x, c = (lax.axis_index(n) for n in ("z", "y", "x", "c"))
    yp, ym = (y + 1) % NY, (y + NY - 1) % NY
    xp, xm = (x + 1) % NX, (x + NX - 1) % NX

    def remote(src, dst, ss, rs, where):
        return pltpu.make_async_remote_copy(
            src_ref=src, dst_ref=dst, send_sem=ss, recv_sem=rs,
            device_id=where, device_id_type=MESH,
        )

    def to_z(s):
        return (z + offset_of(s)) % NZ

    def from_z(s):
        return (z + NZ - offset_of(s)) % NZ

    def zt(s):
        return remote(rows_in.at[to_z(s)], a.at[s, 0], zt_s.at[s], zt_r.at[s], {"z": to_z(s)})

    def zw(s):
        return remote(
            wsend.at[pl.ds(FINE * to_z(s), FINE)], wz.at[s], zw_s.at[s], zw_r.at[s], {"z": to_z(s)}
        )

    def ag(s, j):
        if j == 0:
            src = rows_in.at[z] if isinstance(s, int) and s == 0 else a.at[s, 0]
            dst, where = a.at[s, 1], yp
        elif j == 1:
            src = rows_in.at[z] if isinstance(s, int) and s == 0 else a.at[s, 0]
            dst, where = a.at[s, 3], ym
        elif j == 2:
            src, dst, where = a.at[s, 1, pl.ds(0, HALF)], a.at[s, 2, pl.ds(0, HALF)], yp
        else:
            src, dst, where = a.at[s, 3, pl.ds(HALF, HALF)], a.at[s, 2, pl.ds(HALF, HALF)], ym
        return remote(src, dst, ag_s.at[s, j], ag_r.at[s, j], {"y": where})

    def yw(s, k):
        t = (y + k) % NY
        src = wsend.at[FINE * z + t] if isinstance(s, int) and s == 0 else wz.at[s, t]
        dst = w.at[:, x, NY * from_z(s) + y, c]
        return remote(src, dst, yw_s.at[s, k - 1], yw_r.at[s, k - 1], {"y": t})

    def xw(s, j):
        base = NY * from_z(s)
        if j == 0:
            part, where = w.at[:, x, pl.ds(base, NY), c], xp
        elif j == 1:
            part, where = w.at[:, x, pl.ds(base, NY), c], xm
        elif j == 2:
            part, where = w.at[:, xm, pl.ds(base, 2), c], xp
        else:
            part, where = w.at[:, xp, pl.ds(base + 2, 2), c], xm
        return remote(part, part, xw_s.at[s, j], xw_r.at[s, j], {"x": where})

    def cw(s):
        part = w.at[:, :, pl.ds(NY * from_z(s), NY), c]
        return remote(part, part, cw_s.at[s], cw_r.at[s], {"c": 1 - c})

    def rs(s, j):
        if j == 0:
            src, dst, where = o.at[s, 2, pl.ds(0, HALF)], h.at[s, 0], ym
        elif j == 1:
            src, dst, where = o.at[s, 2, pl.ds(HALF, HALF)], h.at[s, 1], yp
        elif j == 2:
            src, dst, where = o.at[s, 1], f.at[s, 0], ym
        else:
            src, dst, where = o.at[s, 3], f.at[s, 1], yp
        return remote(src, dst, rs_s.at[s, j], rs_r.at[s, j], {"y": where})

    def zb(s):
        return remote(zsum.at[s], back.at[z], zb_s.at[s], zb_r.at[s], {"z": from_z(s)})

    def w_a(s):
        if isinstance(s, int) and s == 0:
            mine = wsend[FINE * z + y]
        else:
            zw(s).wait_recv()
            mine = wz[s, y]
        for k in (1, 3, 2):
            yw(s, k).start()
        w[:, x, NY * from_z(s) + y, c] = mine

    def w_b(s):
        for k in (1, 3, 2):
            yw(s, k).wait_recv()
        xw(s, 0).start()
        xw(s, 1).start()

    def w_c(s):
        xw(s, 0).wait_recv()
        xw(s, 2).start()
        xw(s, 1).wait_recv()
        xw(s, 3).start()

    def w_d(s):
        xw(s, 2).wait_recv()
        xw(s, 3).wait_recv()
        cw(s).start()

    def t_a(s):
        if not (isinstance(s, int) and s == 0):
            zt(s).wait_recv()
        ag(s, 0).start()
        ag(s, 1).start()

    def t_b(s):
        ag(s, 0).wait_recv()
        ag(s, 2).start()
        ag(s, 1).wait_recv()
        ag(s, 3).start()

    def expert(s):
        data = a[s, :, :, 0:D].reshape(NY * ROWS, D)
        extra = a[s, :, :, D:WIDE].reshape(NY * ROWS, LANE).astype(F32)
        lane = lax.broadcasted_iota(jnp.int32, (NY * ROWS, LANE), 1)
        chosen = (lane == y) | (lane == y + FINE)
        scale = jnp.sum(jnp.where(chosen, extra, 0.0), axis=1, keepdims=True)
        acts = []
        for xb in range(NX):
            both = jnp.concatenate(
                [w[0, xb].reshape(D, LANE), w[1, xb].reshape(D, LANE)], axis=1
            )
            r = jnp.dot(data, both, preferred_element_type=F32)
            g, u = r[:, :LANE], r[:, LANE:]
            acts.append((g / (1.0 + jnp.exp(-g)) * u).astype(BF))
        act = jnp.concatenate(acts, axis=1)
        for nb in range(8):
            rhs = jnp.concatenate(
                [w[2, xb, 4 * nb : 4 * nb + 4].reshape(256, LANE) for xb in range(NX)], axis=1
            )
            r = lax.dot_general(
                act, rhs, (((1,), (1,)), ((), ())), preferred_element_type=F32
            )
            r = (r.astype(BF).astype(F32) * scale).astype(BF)
            o[s, :, :, 256 * nb : 256 * nb + 256] = r.reshape(NY, ROWS, 256)

    def t_c(s):
        ag(s, 2).wait_recv()
        ag(s, 3).wait_recv()
        expert(s)
        rs(s, 0).start()
        rs(s, 1).start()

    def t_d(s):
        rs(s, 0).wait_recv()
        o[s, 1, 0:HALF] = (o[s, 1, 0:HALF].astype(F32) + h[s, 0].astype(F32)).astype(BF)
        rs(s, 2).start()
        rs(s, 1).wait_recv()
        o[s, 3, HALF:ROWS] = (o[s, 3, HALF:ROWS].astype(F32) + h[s, 1].astype(F32)).astype(BF)
        rs(s, 3).start()

    def total(s):
        rs(s, 2).wait_recv()
        rs(s, 3).wait_recv()
        return (o[s, 0].astype(F32) + f[s, 0].astype(F32) + f[s, 1].astype(F32)).astype(BF)

    def t_e(s):
        zsum[s] = total(s)
        zb(s).start()

    barrier = pltpu.get_barrier_semaphore()
    peers = (
        [{"z": (z + k) % NZ} for k in range(1, NZ)]
        + [{"y": (y + k) % NY} for k in range(1, NY)]
        + [{"x": (x + k) % NX} for k in range(1, NX)]
        + [{"c": 1 - c}]
    )
    for peer in peers:
        pl.semaphore_signal(barrier, inc=1, device_id=peer, device_id_type=MESH)
    pl.semaphore_wait(barrier, len(peers))

    pair = remote(pieces.at[:, 1 - c], other, pair_s, pair_r, {"c": 1 - c})
    pair.start()
    zt(1).start()
    zt(2).start()
    t_a(0)
    a[0, 0] = rows_in[z]
    pair.wait_recv()

    def join(e, carry):
        mine, theirs = pieces[e, c], other[e]
        low = jnp.where(c == 0, mine, theirs)
        high = jnp.where(c == 0, theirs, mine)
        wsend[e] = jnp.concatenate([low, high], axis=-1)
        return carry

    lax.fori_loop(0, NZ * FINE, join, 0)

    def send_w(s, carry):
        zw(s).start()
        return carry

    lax.fori_loop(1, NZ, send_w, 0)

    def send_t(s, carry):
        zt(s).start()
        return carry

    lax.fori_loop(3, NZ, send_t, 0)

    w_a(0)

    def stage(fn, s):
        pl.when((s >= 0) & (s < NZ))(lambda: fn(s))

    def w_loop(i, carry):
        stage(w_a, i)
        stage(w_b, i - 1)
        stage(w_c, i - 2)
        stage(w_d, i - 3)
        return carry

    lax.fori_loop(1, NZ + 3, w_loop, 0)

    def w_end(s, carry):
        cw(s).wait_recv()
        return carry

    lax.fori_loop(0, NZ, w_end, 0)
    outs = (gate_out, up_out, down_out)
    saves = [
        pltpu.make_async_copy(
            w.at[m, xb], outs[m].at[:, :, :, pl.ds(LANE * xb, LANE)], out_sem.at[m, xb]
        )
        for m in range(3)
        for xb in range(NX)
    ]
    for save in saves:
        save.start()

    def t_loop(i, carry):
        stage(t_a, i)
        stage(t_b, i - 1)
        stage(t_c, i - 2)
        stage(t_d, i - 3)
        pl.when((i >= 5))(lambda: t_e(i - 4))
        pl.when(i == 4)(lambda: keep())
        return carry

    def keep():
        back[z] = total(0)

    lax.fori_loop(1, NZ + 4, t_loop, 0)

    def finish(s, carry):
        zb(s).wait_recv()
        zb(s).wait_send()
        zt(s).wait_send()
        zw(s).wait_send()
        return carry

    lax.fori_loop(1, NZ, finish, 0)

    def drain(s, carry):
        for j in range(4):
            ag(s, j).wait_send()
            xw(s, j).wait_send()
            rs(s, j).wait_send()
        for k in (1, 2, 3):
            yw(s, k).wait_send()
        cw(s).wait_send()
        return carry

    lax.fori_loop(0, NZ, drain, 0)
    pair.wait_send()
    for save in saves:
        save.wait()
    done = pltpu.make_async_copy(back, back_out, back_sem)
    done.start()
    done.wait()


def exchange(outgoing, pieces):
    any_spec = pl.BlockSpec(memory_space=pl.ANY)
    vmem = pl.BlockSpec(memory_space=pltpu.VMEM)
    ready = jax.ShapeDtypeStruct((32, 2, 32, 512), BF)
    dma = pltpu.SemaphoreType.DMA
    scratch = [
        pltpu.VMEM((NZ, NY, ROWS, WIDE), BF),
        pltpu.VMEM((NZ, NY, ROWS, D), BF),
        pltpu.VMEM((NZ, 2, HALF, D), BF),
        pltpu.VMEM((NZ, 2, ROWS, D), BF),
        pltpu.VMEM((NZ, ROWS, D), BF),
        pltpu.VMEM((NZ, ROWS, D), BF),
        pltpu.VMEM((3, NX, 32, 2, 32, LANE), BF),
        pltpu.VMEM((32, 3, 32, LANE), BF),
        pltpu.VMEM((NZ, FINE, 3, 32, LANE), BF),
        pltpu.VMEM((32, 3, 32, 64), BF),
        dma((NZ,)), dma((NZ,)),
        dma((NZ,)), dma((NZ,)),
        dma((NZ, 4)), dma((NZ, 4)),
        dma((NZ, 3)), dma((NZ, 3)),
        dma((NZ, 4)), dma((NZ, 4)),
        dma((NZ,)), dma((NZ,)),
        dma, dma,
        dma((NZ, 4)), dma((NZ, 4)),
        dma((NZ,)), dma((NZ,)),
        dma((3, NX)), dma,
    ]
    return pl.pallas_call(
        kernel,
        out_shape=(jax.ShapeDtypeStruct((NZ, ROWS, D), BF), ready, ready, ready),
        in_specs=[vmem, vmem],
        out_specs=(any_spec,) * 4,
        scratch_shapes=scratch,
        compiler_params=pltpu.CompilerParams(
            collective_id=0, has_side_effects=True, vmem_limit_bytes=56 * 1024 * 1024
        ),
    )(outgoing, pieces)


def local(
    tokens, expert_group, expert_fine, route_weight, norm_gain, gate_master, up_master, down_master
):
    def piece(m):
        return m.astype(BF).reshape(32, 2, 1, 32, 64)

    gain = norm_gain[None, :, None]
    pieces = jnp.concatenate(
        (piece(gain * gate_master), piece(gain * up_master), piece(down_master)), axis=2
    )
    rows, width = tokens.shape
    per_group = rows // NZ
    widened = tokens.astype(F32)
    normed = (
        widened * lax.rsqrt(jnp.mean(widened * widened, axis=-1, keepdims=True) + EPS)
    ).astype(BF)
    same = (expert_group[:, None] == jnp.arange(NZ)[None, :]).astype(BF)
    ahead = jnp.arange(rows)[:, None] > jnp.arange(rows)[None, :]
    before = jnp.dot(ahead.astype(BF), same, preferred_element_type=F32)
    position = jnp.sum(before * same.astype(F32), axis=1).astype(jnp.int32)
    slot = expert_group * per_group + position
    placing = (jnp.arange(rows, dtype=jnp.int32)[:, None] == slot[None, :]).astype(BF)
    fine_weight = jnp.sum(
        jnp.where(
            expert_fine[:, :, None] == jnp.arange(FINE)[None, None, :],
            route_weight[:, :, None],
            0.0,
        ),
        axis=1,
    )
    high = lax.reduce_precision(fine_weight, 8, 7)
    low = (fine_weight - high).astype(BF)
    packed = jnp.concatenate(
        (normed, high.astype(BF), low, jnp.zeros((rows, LANE - 2 * FINE), BF)), axis=1
    )
    outgoing = jnp.dot(placing, packed, preferred_element_type=F32).astype(BF)
    back, gate, up, down = exchange(outgoing.reshape(NZ, per_group, WIDE), pieces)
    mixed = lax.dot_general(
        placing, back.reshape(rows, width), (((0,), (0,)), ((), ())), preferred_element_type=F32
    ).astype(BF)
    return (mixed,) + tuple(r.reshape(1, D, 512) for r in (gate, up, down))


def solution(mesh):
    fine = Mesh(mesh.devices.reshape(NZ, NY, NX, 2), ("z", "y", "x", "c"))
    fs, tp = ("z", "y"), ("x", "c")
    token = fs + tp
    in_specs = (
        P(token, None),
        P(token),
        P(token, None),
        P(token, None),
        P(fs),
        P(None, fs, tp),
        P(None, fs, tp),
        P(None, fs, tp),
    )
    out_specs = (
        P(token, None),
        P(fs, None, None),
        P(fs, None, None),
        P(fs, None, None),
    )
    return jax.shard_map(local, mesh=fine, in_specs=in_specs, out_specs=out_specs, check_vma=False)
```

```python
import jax
import jax.numpy as jnp
from jax import lax
from jax.experimental import pallas as pl
from jax.experimental.pallas import tpu as pltpu
from jax.sharding import Mesh, PartitionSpec as P

FINE = 4
EPS = 1e-06
BF = jnp.bfloat16
F32 = jnp.float32
NZ, NY, NX = 8, 4, 4
ROWS = 32
HALF = 16
D = 2048
LANE = 128
WIDE = D + LANE
MESH = pl.DeviceIdType.MESH


def offset_of(s):
    far = (s + 1) // 2
    odd = s % 2
    return (odd * far + (1 - odd) * (NZ - far)) % NZ


def placing_of(group):
    count = NZ * ROWS
    lane = lax.broadcasted_iota(jnp.int32, (count, count), 1)
    sub = lax.broadcasted_iota(jnp.int32, (count, count), 0)
    same = lax.broadcasted_iota(jnp.int32, (16, count), 0) == group
    same = jnp.where(same, 1.0, 0.0)
    earlier = jnp.where(sub < lane, 1.0, 0.0).astype(BF)
    before = jnp.dot(same.astype(BF), earlier, preferred_element_type=F32)
    position = jnp.sum(before * same, axis=0, keepdims=True)
    slot = group.astype(F32) * ROWS + position
    return jnp.where(sub.astype(F32) == slot, 1.0, 0.0).astype(BF)


def kernel(
    tokens_in, group_in, fine_in, route_in, gain_in, gate_in, up_in, down_in,
    back_out, gate_out, up_out, down_out,
    tok, masters, normed, rows_in, pieces,
    a, o, h, f, zsum, back, w, wsend, wz, other,
    load_sem,
    zt_s, zt_r, zw_s, zw_r, ag_s, ag_r, yw_s, yw_r, xw_s, xw_r, cw_s, cw_r,
    pair_s, pair_r, rs_s, rs_r, zb_s, zb_r, out_sem, back_sem,
):
    z, y, x, c = (lax.axis_index(n) for n in ("z", "y", "x", "c"))
    yp, ym = (y + 1) % NY, (y + NY - 1) % NY
    xp, xm = (x + 1) % NX, (x + NX - 1) % NX

    def remote(src, dst, ss, rs, where):
        return pltpu.make_async_remote_copy(
            src_ref=src, dst_ref=dst, send_sem=ss, recv_sem=rs,
            device_id=where, device_id_type=MESH,
        )

    def to_z(s):
        return (z + offset_of(s)) % NZ

    def from_z(s):
        return (z + NZ - offset_of(s)) % NZ

    def zt(s):
        return remote(rows_in.at[to_z(s)], a.at[s, 0], zt_s.at[s], zt_r.at[s], {"z": to_z(s)})

    def zw(s):
        return remote(
            wsend.at[pl.ds(FINE * to_z(s), FINE)], wz.at[s], zw_s.at[s], zw_r.at[s], {"z": to_z(s)}
        )

    def ag(s, j):
        if j == 0:
            src = rows_in.at[z] if isinstance(s, int) and s == 0 else a.at[s, 0]
            dst, where = a.at[s, 1], yp
        elif j == 1:
            src = rows_in.at[z] if isinstance(s, int) and s == 0 else a.at[s, 0]
            dst, where = a.at[s, 3], ym
        elif j == 2:
            src, dst, where = a.at[s, 1, pl.ds(0, HALF)], a.at[s, 2, pl.ds(0, HALF)], yp
        else:
            src, dst, where = a.at[s, 3, pl.ds(HALF, HALF)], a.at[s, 2, pl.ds(HALF, HALF)], ym
        return remote(src, dst, ag_s.at[s, j], ag_r.at[s, j], {"y": where})

    def yw(s, k):
        t = (y + k) % NY
        src = wsend.at[FINE * z + t] if isinstance(s, int) and s == 0 else wz.at[s, t]
        dst = w.at[:, x, NY * from_z(s) + y, c]
        return remote(src, dst, yw_s.at[s, k - 1], yw_r.at[s, k - 1], {"y": t})

    def xw(s, j):
        base = NY * from_z(s)
        if j == 0:
            part, where = w.at[:, x, pl.ds(base, NY), c], xp
        elif j == 1:
            part, where = w.at[:, x, pl.ds(base, NY), c], xm
        elif j == 2:
            part, where = w.at[:, xm, pl.ds(base, 2), c], xp
        else:
            part, where = w.at[:, xp, pl.ds(base + 2, 2), c], xm
        return remote(part, part, xw_s.at[s, j], xw_r.at[s, j], {"x": where})

    def cw(s):
        part = w.at[:, :, pl.ds(NY * from_z(s), NY), c]
        return remote(part, part, cw_s.at[s], cw_r.at[s], {"c": 1 - c})

    def rs(s, j):
        if j == 0:
            src, dst, where = o.at[s, 2, pl.ds(0, HALF)], h.at[s, 0], ym
        elif j == 1:
            src, dst, where = o.at[s, 2, pl.ds(HALF, HALF)], h.at[s, 1], yp
        elif j == 2:
            src, dst, where = o.at[s, 1], f.at[s, 0], ym
        else:
            src, dst, where = o.at[s, 3], f.at[s, 1], yp
        return remote(src, dst, rs_s.at[s, j], rs_r.at[s, j], {"y": where})

    def zb(s):
        return remote(zsum.at[s], back.at[z], zb_s.at[s], zb_r.at[s], {"z": from_z(s)})

    def w_a(s):
        if isinstance(s, int) and s == 0:
            mine = wsend[FINE * z + y]
        else:
            zw(s).wait_recv()
            mine = wz[s, y]
        for k in (1, 3, 2):
            yw(s, k).start()
        w[:, x, NY * from_z(s) + y, c] = mine

    def w_b(s):
        for k in (1, 3, 2):
            yw(s, k).wait_recv()
        xw(s, 0).start()
        xw(s, 1).start()

    def w_c(s):
        xw(s, 0).wait_recv()
        xw(s, 2).start()
        xw(s, 1).wait_recv()
        xw(s, 3).start()

    def w_d(s):
        xw(s, 2).wait_recv()
        xw(s, 3).wait_recv()
        cw(s).start()

    def t_a(s):
        if not (isinstance(s, int) and s == 0):
            zt(s).wait_recv()
        ag(s, 0).start()
        ag(s, 1).start()

    def t_b(s):
        ag(s, 0).wait_recv()
        ag(s, 2).start()
        ag(s, 1).wait_recv()
        ag(s, 3).start()

    def expert(s):
        data = a[s, :, :, 0:D].reshape(NY * ROWS, D)
        extra = a[s, :, :, D:WIDE].reshape(NY * ROWS, LANE).astype(F32)
        lane = lax.broadcasted_iota(jnp.int32, (NY * ROWS, LANE), 1)
        chosen = (lane == y) | (lane == y + FINE)
        scale = jnp.sum(jnp.where(chosen, extra, 0.0), axis=1, keepdims=True)
        acts = []
        for xb in range(NX):
            both = jnp.concatenate(
                [w[0, xb].reshape(D, LANE), w[1, xb].reshape(D, LANE)], axis=1
            )
            r = jnp.dot(data, both, preferred_element_type=F32)
            g, u = r[:, :LANE], r[:, LANE:]
            acts.append((g / (1.0 + jnp.exp(-g)) * u).astype(BF))
        act = jnp.concatenate(acts, axis=1)
        for nb in range(8):
            rhs = jnp.concatenate(
                [w[2, xb, 4 * nb : 4 * nb + 4].reshape(256, LANE) for xb in range(NX)], axis=1
            )
            r = lax.dot_general(
                act, rhs, (((1,), (1,)), ((), ())), preferred_element_type=F32
            )
            r = (r.astype(BF).astype(F32) * scale).astype(BF)
            o[s, :, :, 256 * nb : 256 * nb + 256] = r.reshape(NY, ROWS, 256)

    def t_c(s):
        ag(s, 2).wait_recv()
        ag(s, 3).wait_recv()
        with jax.named_scope("expert"):
            expert(s)
        rs(s, 0).start()
        rs(s, 1).start()

    def t_d(s):
        rs(s, 0).wait_recv()
        o[s, 1, 0:HALF] = (o[s, 1, 0:HALF].astype(F32) + h[s, 0].astype(F32)).astype(BF)
        rs(s, 2).start()
        rs(s, 1).wait_recv()
        o[s, 3, HALF:ROWS] = (o[s, 3, HALF:ROWS].astype(F32) + h[s, 1].astype(F32)).astype(BF)
        rs(s, 3).start()

    def total(s):
        rs(s, 2).wait_recv()
        rs(s, 3).wait_recv()
        return (o[s, 0].astype(F32) + f[s, 0].astype(F32) + f[s, 1].astype(F32)).astype(BF)

    def t_e(s):
        zsum[s] = total(s)
        pl.when(s > 0)(lambda: zb(s).start())

    loads = [
        pltpu.make_async_copy(src, dst, load_sem.at[k])
        for k, (src, dst) in enumerate(
            (
                (tokens_in, tok),
                (gate_in, masters.at[0]),
                (up_in, masters.at[1]),
                (down_in, masters.at[2]),
            )
        )
    ]
    for load in loads[1:]:
        load.start()
    loads[0].start()
    barrier = pltpu.get_barrier_semaphore()
    peers = (
        [{"z": (z + k) % NZ} for k in range(1, NZ)]
        + [{"y": (y + k) % NY} for k in range(1, NY)]
        + [{"x": (x + k) % NX} for k in range(1, NX)]
        + [{"c": 1 - c}]
    )
    for peer in peers:
        pl.semaphore_signal(barrier, inc=1, device_id=peer, device_id_type=MESH)
    pair = remote(pieces.at[1 - c], other, pair_s, pair_r, {"c": 1 - c})

    for load in loads[1:]:
        load.wait()
    eye = lax.broadcasted_iota(jnp.int32, (64, 64), 0) == lax.broadcasted_iota(
        jnp.int32, (64, 64), 1
    )
    gain = jnp.sum(jnp.where(eye, gain_in[...], 0.0), axis=1, keepdims=True)

    def cast(e, carry):
        for m in range(3):
            value = masters[m, e] if m == 2 else gain * masters[m, e]
            value = value.astype(BF)
            pieces[0, e, m] = value[:32]
            pieces[1, e, m] = value[32:]
        return carry

    with jax.named_scope("cast"):
        lax.fori_loop(0, NZ * FINE, cast, 0, unroll=4)
    with jax.named_scope("barrier"):
        pl.semaphore_wait(barrier, len(peers))
    pair.start()

    loads[0].wait()

    def norm(r, carry):
        wide = tok[pl.ds(pl.multiple_of(r * ROWS, ROWS), ROWS), :].astype(F32)
        mean = jnp.sum(wide * wide, axis=1, keepdims=True) * (1.0 / D)
        normed[pl.ds(pl.multiple_of(r * ROWS, ROWS), ROWS), :] = (
            wide * lax.rsqrt(mean + EPS)
        ).astype(BF)
        return carry

    with jax.named_scope("norm"):
        lax.fori_loop(0, NZ, norm, 0)
        count = NZ * ROWS
        placing = placing_of(group_in[...])
        entry = lax.broadcasted_iota(jnp.int32, (8, count), 0)
        fine_id = entry % FINE
        weight = jnp.where(fine_in[0:1] == fine_id, route_in[0:1], 0.0) + jnp.where(
            fine_in[1:2] == fine_id, route_in[1:2], 0.0
        )
        top = weight.astype(BF).astype(F32)
        weight = jnp.where(entry < FINE, top, weight - top)
        weight = jnp.concatenate([weight, jnp.zeros((LANE - 8, count), F32)], axis=0).astype(BF)
        extra = lax.dot_general(
            placing, weight, (((1,), (1,)), ((), ())), preferred_element_type=F32
        )
        rows_in[:, :, D:WIDE] = extra.astype(BF).reshape(NZ, ROWS, LANE)
        for nb in range(8):
            part = jnp.dot(
                placing, normed[:, 256 * nb : 256 * nb + 256], preferred_element_type=F32
            )
            rows_in[:, :, 256 * nb : 256 * nb + 256] = part.astype(BF).reshape(NZ, ROWS, 256)

    zt(1).start()
    zt(2).start()
    t_a(0)
    with jax.named_scope("pair"):
        pair.wait_recv()

    def join(e, carry):
        mine, theirs = pieces[c, e], other[e]
        low = jnp.where(c == 0, mine, theirs)
        high = jnp.where(c == 0, theirs, mine)
        wsend[e] = jnp.concatenate([low, high], axis=-1)
        return carry

    with jax.named_scope("join"):
        lax.fori_loop(0, NZ * FINE, join, 0, unroll=4)

    w_a(0)

    def send_w(s, carry):
        zw(s).start()
        return carry

    lax.fori_loop(1, NZ, send_w, 0)

    def send_t(s, carry):
        zt(s).start()
        return carry

    lax.fori_loop(3, NZ, send_t, 0)
    a[0, 0] = rows_in[z]

    def run(fn, s):
        with jax.named_scope(fn.__name__):
            fn(s)

    def stage(fn, s):
        pl.when((s >= 0) & (s < NZ))(lambda: run(fn, s))

    def at(i, when, fn, s):
        pl.when(i == when)(lambda: run(fn, s))

    def w_loop(i, carry):
        stage(w_b, i - 1)
        at(i, 1, t_a, 1)
        stage(w_a, i)
        at(i, 2, t_b, 0)
        stage(w_c, i - 2)
        at(i, 3, t_a, 2)
        at(i, 4, t_b, 1)
        stage(w_d, i - 3)
        at(i, 6, t_b, 2)
        at(i, 8, t_a, 3)
        at(i, 9, t_a, 4)
        at(i, 10, t_b, 3)
        return carry

    lax.fori_loop(1, NZ + 3, w_loop, 0)

    def w_end(s, carry):
        with jax.named_scope("w_end"):
            cw(s).wait_recv()
        return carry

    lax.fori_loop(0, NZ, w_end, 0)
    outs = (gate_out, up_out, down_out)
    saves = [
        pltpu.make_async_copy(
            w.at[m, xb], outs[m].at[:, :, :, pl.ds(LANE * xb, LANE)], out_sem.at[m, xb]
        )
        for m in range(3)
        for xb in range(NX)
    ]
    for save in saves:
        save.start()

    def slot(i):
        return (i + 1) % NZ

    def t_loop(i, carry):
        pl.when(i < 3)(lambda: run(t_a, i + 5))
        pl.when(i < 4)(lambda: run(t_b, i + 4))
        pl.when(i < NZ)(lambda: run(t_c, slot(i)))
        pl.when((i >= 1) & (i < NZ + 1))(lambda: run(t_d, slot(i - 1)))
        pl.when(i >= 2)(lambda: run(t_e, slot(i - 2)))

        @pl.when(i < NZ)
        def _():
            s = i
            for j in range(4):
                xw(s, j).wait_send()
            for k in (1, 2, 3):
                yw(s, k).wait_send()
            cw(s).wait_send()

        @pl.when((i >= 1) & (i < NZ))
        def _():
            zw(i).wait_send()
            zt(i).wait_send()

        return carry

    lax.fori_loop(0, NZ + 2, t_loop, 0)
    back[z] = zsum[0]

    def drain(s, carry):
        for j in range(4):
            ag(s, j).wait_send()
            rs(s, j).wait_send()
        return carry

    lax.fori_loop(0, NZ, drain, 0)
    pair.wait_send()
    for save in saves:
        save.wait()

    def finish(s, carry):
        with jax.named_scope("finish"):
            zb(s).wait_recv()
        zb(s).wait_send()
        return carry

    lax.fori_loop(1, NZ, finish, 0)
    done = pltpu.make_async_copy(back, back_out, back_sem)
    done.start()
    done.wait()


def settle(back_in, group_in, g_in, u_in, d_in, mixed_out, g_out, u_out, d_out,
           back, mixed, hold, back_sem, in_sem, out_sem, mixed_sem):
    first = pltpu.make_async_copy(back_in, back, back_sem)
    first.start()
    ins, outs = (g_in, u_in, d_in), (g_out, u_out, d_out)
    parts = [(m, p) for m in range(3) for p in range(2)]
    reads = [
        pltpu.make_async_copy(
            ins[m].at[pl.ds(D // 2 * p, D // 2)], hold.at[m, p], in_sem.at[m, p]
        )
        for m, p in parts
    ]
    writes = [
        pltpu.make_async_copy(
            hold.at[m, p], outs[m].at[pl.ds(D // 2 * p, D // 2)], out_sem.at[m, p]
        )
        for m, p in parts
    ]
    for read in reads:
        read.start()
    placing = placing_of(group_in[...])
    first.wait()
    results = []
    for nb in range(4):
        for k in ((0, 1), (2,), (3, 4), (5,))[nb]:
            reads[k].wait()
            writes[k].start()
        cols = pl.ds(512 * nb, 512)
        mixed[:, cols] = lax.dot_general(
            placing, back[:, cols], (((0,), (0,)), ((), ())), preferred_element_type=F32
        ).astype(BF)
    last = pltpu.make_async_copy(mixed, mixed_out, mixed_sem)
    last.start()
    for write in writes:
        write.wait()
    last.wait()


def exchange(tokens, group, fine, route, gain, gate, up, down):
    any_spec = pl.BlockSpec(memory_space=pl.ANY)
    vmem = pl.BlockSpec(memory_space=pltpu.VMEM)
    ready = jax.ShapeDtypeStruct((32, 2, 32, 512), BF)
    dma = pltpu.SemaphoreType.DMA
    count = NZ * ROWS
    scratch = [
        pltpu.VMEM((count, D), BF),
        pltpu.VMEM((3, 32, 64, 64), F32),
        pltpu.VMEM((count, D), BF),
        pltpu.VMEM((NZ, ROWS, WIDE), BF),
        pltpu.VMEM((2, 32, 3, 32, 64), BF),
        pltpu.VMEM((NZ, NY, ROWS, WIDE), BF),
        pltpu.VMEM((NZ, NY, ROWS, D), BF),
        pltpu.VMEM((NZ, 2, HALF, D), BF),
        pltpu.VMEM((NZ, 2, ROWS, D), BF),
        pltpu.VMEM((NZ, ROWS, D), BF),
        pltpu.VMEM((NZ, ROWS, D), BF),
        pltpu.VMEM((3, NX, 32, 2, 32, LANE), BF),
        pltpu.VMEM((32, 3, 32, LANE), BF),
        pltpu.VMEM((NZ, FINE, 3, 32, LANE), BF),
        pltpu.VMEM((32, 3, 32, 64), BF),
        dma((4,)),
        dma((NZ,)), dma((NZ,)),
        dma((NZ,)), dma((NZ,)),
        dma((NZ, 4)), dma((NZ, 4)),
        dma((NZ, 3)), dma((NZ, 3)),
        dma((NZ, 4)), dma((NZ, 4)),
        dma((NZ,)), dma((NZ,)),
        dma, dma,
        dma((NZ, 4)), dma((NZ, 4)),
        dma((NZ,)), dma((NZ,)),
        dma((3, NX)), dma,
    ]
    back, *ready = pl.pallas_call(
        kernel,
        out_shape=(jax.ShapeDtypeStruct((NZ, ROWS, D), BF), ready, ready, ready),
        in_specs=[any_spec, vmem, vmem, vmem, vmem, any_spec, any_spec, any_spec],
        out_specs=(any_spec,) * 4,
        scratch_shapes=scratch,
        compiler_params=pltpu.CompilerParams(
            collective_id=0, has_side_effects=True, vmem_limit_bytes=56 * 1024 * 1024
        ),
    )(tokens, group, fine, route, gain, gate, up, down)
    mixed = jax.ShapeDtypeStruct((count, D), BF)
    flat = jax.ShapeDtypeStruct((D, 512), BF)
    return pl.pallas_call(
        settle,
        out_shape=(mixed, flat, flat, flat),
        in_specs=[any_spec, vmem, any_spec, any_spec, any_spec],
        out_specs=(any_spec,) * 4,
        scratch_shapes=[
            pltpu.VMEM((count, D), BF),
            pltpu.VMEM((count, D), BF),
            pltpu.VMEM((3, 2, D // 2, 512), BF),
            dma, dma((3, 2)), dma((3, 2)), dma,
        ],
        compiler_params=pltpu.CompilerParams(vmem_limit_bytes=56 * 1024 * 1024),
    )(back.reshape(count, D), group, *(r.reshape(D, 512) for r in ready))


def local(
    tokens, expert_group, expert_fine, route_weight, norm_gain, gate_master, up_master, down_master
):
    mixed, gate, up, down = exchange(
        tokens,
        expert_group.reshape(1, -1),
        expert_fine.T,
        route_weight.T,
        norm_gain.reshape(1, -1),
        gate_master,
        up_master,
        down_master,
    )
    return (mixed,) + tuple(r.reshape(1, D, 512) for r in (gate, up, down))


def solution(mesh):
    fine = Mesh(mesh.devices.reshape(NZ, NY, NX, 2), ("z", "y", "x", "c"))
    fs, tp = ("z", "y"), ("x", "c")
    token = fs + tp
    in_specs = (
        P(token, None),
        P(token),
        P(token, None),
        P(token, None),
        P(fs),
        P(None, fs, tp),
        P(None, fs, tp),
        P(None, fs, tp),
    )
    out_specs = (
        P(token, None),
        P(fs, None, None),
        P(fs, None, None),
        P(fs, None, None),
    )
    return jax.shard_map(local, mesh=fine, in_specs=in_specs, out_specs=out_specs, check_vma=False)
```

```python
import jax
import jax.numpy as jnp
from jax import lax
from jax.experimental import pallas as pl
from jax.experimental.pallas import tpu as pltpu
from jax.sharding import Mesh, PartitionSpec as P

FINE = 4
EPS = 1e-06
BF = jnp.bfloat16
F32 = jnp.float32
NZ, NY, NX = 8, 4, 4
ROWS = 32
HALF = 16
D = 2048
LANE = 128
MESH = pl.DeviceIdType.MESH


def offset_of(s):
    far = (s + 1) // 2
    odd = s % 2
    return (odd * far + (1 - odd) * (NZ - far)) % NZ


def token_offset_of(k):
    late = (k + 3) // 8
    return (NZ + 4 * late + (2 * (k % 2) - 1) * ((k + 1 - 5 * late) // 2)) % NZ


def placing_of(group):
    count = NZ * ROWS
    lane = lax.broadcasted_iota(jnp.int32, (count, count), 1)
    sub = lax.broadcasted_iota(jnp.int32, (count, count), 0)
    same = lax.broadcasted_iota(jnp.int32, (16, count), 0) == group
    same = jnp.where(same, 1.0, 0.0)
    earlier = jnp.where(sub < lane, 1.0, 0.0).astype(BF)
    before = jnp.dot(same.astype(BF), earlier, preferred_element_type=F32)
    position = jnp.sum(before * same, axis=0, keepdims=True)
    slot = group.astype(F32) * ROWS + position
    return jnp.where(sub.astype(F32) == slot, 1.0, 0.0).astype(BF)


def kernel(
    tokens_in, group_in, fine_in, route_in, gain_in, gate_in, up_in, down_in,
    back, w,
    tok, masters, normed, rows_in, pieces, scales, near,
    a, o, h, f, zsum, wsend, other,
    load_sem, wt_s, wt_r,
    zt_s, zt_r, ws_s, ws_r, ag_s, ag_r, xw_s, xw_r, cw_s, cw_r,
    pair_s, pair_r, rs_s, rs_r, zb_s, zb_r,
):
    z, y, x, c = (lax.axis_index(n) for n in ("z", "y", "x", "c"))
    yp, ym = (y + 1) % NY, (y + NY - 1) % NY
    xp, xm = (x + 1) % NX, (x + NX - 1) % NX

    def remote(src, dst, ss, rs, where):
        return pltpu.make_async_remote_copy(
            src_ref=src, dst_ref=dst, send_sem=ss, recv_sem=rs,
            device_id=where, device_id_type=MESH,
        )

    def to_z(s):
        return (z + offset_of(s)) % NZ

    def from_z(s):
        return (z + NZ - offset_of(s)) % NZ

    def token_to_z(k):
        return (z + token_offset_of(k)) % NZ

    def token_from_z(k):
        return (z + NZ - token_offset_of(k)) % NZ

    def zt(k):
        t = token_to_z(k)
        return remote(rows_in.at[t], a.at[k, 0], zt_s.at[k], zt_r.at[k], {"z": t})

    def ws(s, k):
        tz, ty = to_z(s), (y + k) % NY
        return remote(
            wsend.at[FINE * tz + ty], w.at[:, x, NY * z + y, c],
            ws_s.at[s, k], ws_r.at[s, k], {"z": tz, "y": ty},
        )

    def wt(k, j):
        tz, ty = token_to_z(k), (y + j) % NY
        return remote(
            scales.at[ty, tz // 4], near.at[k, j], wt_s.at[k, j], wt_r.at[k, j],
            {"z": tz, "y": ty},
        )

    def ag(s, j):
        if j == 0:
            src = rows_in.at[z] if isinstance(s, int) and s == 0 else a.at[s, 0]
            dst, where = a.at[s, 1], yp
        elif j == 1:
            src = rows_in.at[z] if isinstance(s, int) and s == 0 else a.at[s, 0]
            dst, where = a.at[s, 3], ym
        elif j == 2:
            src, dst, where = a.at[s, 1, pl.ds(0, HALF)], a.at[s, 2, pl.ds(0, HALF)], yp
        else:
            src, dst, where = a.at[s, 3, pl.ds(HALF, HALF)], a.at[s, 2, pl.ds(HALF, HALF)], ym
        return remote(src, dst, ag_s.at[s, j], ag_r.at[s, j], {"y": where})

    def xw(s, j):
        base = NY * from_z(s)
        if j == 0:
            part, where = w.at[:, x, pl.ds(base, NY), c], xp
        elif j == 1:
            part, where = w.at[:, x, pl.ds(base, NY), c], xm
        elif j == 2:
            part, where = w.at[:, xm, pl.ds(base, 2), c], xp
        else:
            part, where = w.at[:, xp, pl.ds(base + 2, 2), c], xm
        return remote(part, part, xw_s.at[s, j], xw_r.at[s, j], {"x": where})

    def cw(s):
        part = w.at[:, :, pl.ds(NY * from_z(s), NY), c]
        return remote(part, part, cw_s.at[s], cw_r.at[s], {"c": 1 - c})

    def rs(s, j):
        if j == 0:
            src, dst, where = o.at[s, 2, pl.ds(0, HALF)], h.at[s, 0], ym
        elif j == 1:
            src, dst, where = o.at[s, 2, pl.ds(HALF, HALF)], h.at[s, 1], yp
        elif j == 2:
            src, dst, where = o.at[s, 1], f.at[s, 0], ym
        else:
            src, dst, where = o.at[s, 3], f.at[s, 1], yp
        return remote(src, dst, rs_s.at[s, j], rs_r.at[s, j], {"y": where})

    def zb(s):
        return remote(zsum.at[s], back.at[z], zb_s.at[s], zb_r.at[s], {"z": token_from_z(s)})

    def w_b(s):
        for k in range(1, NY):
            ws(s, k).wait_recv()
        pl.when(s > 0)(lambda: ws(s, 0).wait_recv())
        xw(s, 0).start()
        xw(s, 1).start()

    def w_c(s):
        xw(s, 0).wait_recv()
        xw(s, 2).start()
        xw(s, 1).wait_recv()
        xw(s, 3).start()

    def w_d(s):
        xw(s, 2).wait_recv()
        xw(s, 3).wait_recv()
        cw(s).start()

    def t_a(s):
        if not (isinstance(s, int) and s == 0):
            zt(s).wait_recv()
        ag(s, 0).start()
        ag(s, 1).start()

    def t_b(s):
        ag(s, 0).wait_recv()
        ag(s, 2).start()
        ag(s, 1).wait_recv()
        ag(s, 3).start()

    def expert(s):
        data = a[s].reshape(NY * ROWS, D)
        lane = lax.broadcasted_iota(jnp.int32, (ROWS, LANE), 1)
        row = lax.broadcasted_iota(jnp.int32, (ROWS, LANE), 0)
        mine = lane == row + ROWS * (z % 4)
        scale = jnp.concatenate(
            [
                jnp.sum(jnp.where(mine, near[s, j], 0.0), axis=1, keepdims=True)
                for j in range(NY)
            ],
            axis=0,
        )
        acts = []
        for xb in range(NX):
            both = jnp.concatenate(
                [w[0, xb].reshape(D, LANE), w[1, xb].reshape(D, LANE)], axis=1
            )
            r = jnp.dot(data, both, preferred_element_type=F32)
            g, u = r[:, :LANE], r[:, LANE:]
            acts.append((g / (1.0 + jnp.exp(-g)) * u).astype(BF))
        act = jnp.concatenate(acts, axis=1)
        for nb in range(8):
            rhs = jnp.concatenate(
                [w[2, xb, 4 * nb : 4 * nb + 4].reshape(256, LANE) for xb in range(NX)], axis=1
            )
            r = lax.dot_general(
                act, rhs, (((1,), (1,)), ((), ())), preferred_element_type=F32
            )
            r = (r.astype(BF).astype(F32) * scale).astype(BF)
            o[s, :, :, 256 * nb : 256 * nb + 256] = r.reshape(NY, ROWS, 256)

    def t_c(s):
        for j in range(1, NY):
            wt(s, j).wait_recv()
        pl.when(s > 0)(lambda: wt(s, 0).wait_recv())
        ag(s, 2).wait_recv()
        ag(s, 3).wait_recv()
        with jax.named_scope("expert"):
            expert(s)
        rs(s, 0).start()
        rs(s, 1).start()

    def t_d(s):
        rs(s, 0).wait_recv()
        o[s, 1, 0:HALF] = (o[s, 1, 0:HALF].astype(F32) + h[s, 0].astype(F32)).astype(BF)
        rs(s, 2).start()
        rs(s, 1).wait_recv()
        o[s, 3, HALF:ROWS] = (o[s, 3, HALF:ROWS].astype(F32) + h[s, 1].astype(F32)).astype(BF)
        rs(s, 3).start()

    def total(s):
        rs(s, 2).wait_recv()
        rs(s, 3).wait_recv()
        return (o[s, 0].astype(F32) + f[s, 0].astype(F32) + f[s, 1].astype(F32)).astype(BF)

    def t_e(s):
        zsum[s] = total(s)
        pl.when(s > 0)(lambda: zb(s).start())
        for j in range(4):
            rs(s, j).wait_send()

    loads = [
        pltpu.make_async_copy(src, dst, load_sem.at[k])
        for k, (src, dst) in enumerate(
            (
                (tokens_in, tok),
                (gate_in, masters.at[0]),
                (up_in, masters.at[1]),
                (down_in, masters.at[2]),
            )
        )
    ]
    for load in loads[1:]:
        load.start()
    loads[0].start()
    barrier = pltpu.get_barrier_semaphore()
    peers = [{"x": (x + k) % NX} for k in range(1, NX)] + [{"c": 1 - c}]
    for peer in peers:
        pl.semaphore_signal(barrier, inc=1, device_id=peer, device_id_type=MESH)

    def greet(q, carry):
        peer = {"z": (z + q // NY) % NZ, "y": (y + q % NY) % NY}
        pl.semaphore_signal(barrier, inc=1, device_id=peer, device_id_type=MESH)
        return carry

    lax.fori_loop(1, NZ * NY, greet, 0)

    pair = remote(pieces.at[1 - c], other, pair_s, pair_r, {"c": 1 - c})

    for load in loads[1:]:
        load.wait()
    eye = lax.broadcasted_iota(jnp.int32, (64, 64), 0) == lax.broadcasted_iota(
        jnp.int32, (64, 64), 1
    )
    gain = jnp.sum(jnp.where(eye, gain_in[...], 0.0), axis=1, keepdims=True)

    def cast(e, carry):
        for m in range(3):
            value = masters[m, e] if m == 2 else gain * masters[m, e]
            value = value.astype(BF)
            pieces[0, e, m] = value[:32]
            pieces[1, e, m] = value[32:]
        return carry

    with jax.named_scope("cast"):
        lax.fori_loop(0, NZ * FINE, cast, 0, unroll=4)
    with jax.named_scope("barrier"):
        pl.semaphore_wait(barrier, NZ * NY - 1 + len(peers))
    pair.start()

    loads[0].wait()

    def norm(r, carry):
        wide = tok[pl.ds(pl.multiple_of(r * ROWS, ROWS), ROWS), :].astype(F32)
        mean = jnp.sum(wide * wide, axis=1, keepdims=True) * (1.0 / D)
        normed[pl.ds(pl.multiple_of(r * ROWS, ROWS), ROWS), :] = (
            wide * lax.rsqrt(mean + EPS)
        ).astype(BF)
        return carry

    with jax.named_scope("norm"):
        lax.fori_loop(0, NZ, norm, 0)
        count = NZ * ROWS
        placing = placing_of(group_in[...])
        entry = lax.broadcasted_iota(jnp.int32, (8, count), 0)
        fine_id = entry % FINE
        weight = jnp.where(fine_in[0:1] == fine_id, route_in[0:1], 0.0) + jnp.where(
            fine_in[1:2] == fine_id, route_in[1:2], 0.0
        )
        top = weight.astype(BF).astype(F32)
        weight = jnp.where(entry < FINE, top, weight - top)
        weight = jnp.concatenate([weight, jnp.zeros((8, count), F32)], axis=0).astype(BF)
        sorted_weight = lax.dot_general(
            weight, placing, (((1,), (1,)), ((), ())), preferred_element_type=F32
        )
        sorted_weight = sorted_weight[0:FINE] + sorted_weight[FINE : 2 * FINE]
        for e in range(FINE):
            for p in range(2):
                scales[e, p] = sorted_weight[e : e + 1, LANE * p : LANE * p + LANE]
        for nb in range(8):
            part = jnp.dot(
                placing, normed[:, 256 * nb : 256 * nb + 256], preferred_element_type=F32
            )
            rows_in[:, :, 256 * nb : 256 * nb + 256] = part.astype(BF).reshape(NZ, ROWS, 256)

    with jax.named_scope("pair"):
        pair.wait_recv()

    def join(e, carry):
        mine, theirs = pieces[c, e], other[e]
        low = jnp.where(c == 0, mine, theirs)
        high = jnp.where(c == 0, theirs, mine)
        wsend[e] = jnp.concatenate([low, high], axis=-1)
        return carry

    with jax.named_scope("join"):
        lax.fori_loop(0, NZ * FINE, join, 0, unroll=4)

    def send(copy, first, last):
        def one(s, carry):
            copy(s)
            return carry

        lax.fori_loop(first, last, one, 0)

    def send_w(s):
        for k in (1, 3, 2, 0):
            ws(s, k).start()

    def send_t(k):
        zt(k).start()
        for j in range(NY):
            wt(k, j).start()

    for k in (1, 3, 2):
        ws(0, k).start()
    w[:, x, NY * z + y, c] = wsend[FINE * z + y]
    send(send_w, 1, 3)
    send(send_t, 1, 3)
    t_a(0)
    send(send_w, 3, NZ)
    send(send_t, 3, NZ)
    for j in range(1, NY):
        wt(0, j).start()
    near[0, 0] = scales[y, z // 4]
    a[0, 0] = rows_in[z]

    def run(fn, s):
        with jax.named_scope(fn.__name__):
            fn(s)

    def at(i, when, *todo):
        @pl.when(i == when)
        def _():
            for fn, s in todo:
                run(fn, s)

    run(w_b, 0)
    run(w_b, 1)
    run(t_a, 1)

    def w_loop(i, carry):
        pl.when(i < NZ - 2)(lambda: run(w_b, i + 2))
        at(i, 0, (t_b, 0))
        pl.when(i < NZ)(lambda: run(w_c, i))
        at(i, 0, (t_a, 2))
        pl.when(i >= 2)(lambda: run(w_d, i - 2))
        at(i, 2, (t_b, 1))
        at(i, 4, (t_b, 2))
        at(i, 5, (t_a, 3), (t_a, 4))
        at(i, 8, (t_b, 3))
        at(i, 9, (t_a, 5), (t_b, 4))
        return carry

    lax.fori_loop(0, NZ + 2, w_loop, 0)

    def w_end(s, carry):
        with jax.named_scope("w_end"):
            cw(s).wait_recv()
        return carry

    lax.fori_loop(0, NZ, w_end, 0)
    order = 0o02765143

    def t_loop(i, carry):
        now, before, last = carry
        at(i, 4, (t_b, 7))
        pl.when(i < NZ)(lambda: run(t_c, now % 8))
        pl.when((i >= 1) & (i < NZ + 1))(lambda: run(t_d, before % 8))
        at(i, 1, (t_b, 5))
        at(i, 2, (t_a, 6), (t_a, 7))
        pl.when(i >= 2)(lambda: run(t_e, last % 8))
        at(i, 3, (t_b, 6))

        @pl.when(i < NZ)
        def _():
            s = i
            for j in range(4):
                xw(s, j).wait_send()
                ag(s, j).wait_send()
            for k in (1, 2, 3):
                ws(s, k).wait_send()
                wt(s, k).wait_send()
            cw(s).wait_send()

        @pl.when((i >= 1) & (i < NZ))
        def _():
            ws(i, 0).wait_send()
            wt(i, 0).wait_send()
            zt(i).wait_send()

        return now // 8, now, before

    lax.fori_loop(0, NZ + 2, t_loop, (jnp.int32(order), jnp.int32(0), jnp.int32(0)))
    back[z] = zsum[0]

    pair.wait_send()

    def finish(s, carry):
        with jax.named_scope("finish"):
            zb(s).wait_recv()
        zb(s).wait_send()
        return carry

    lax.fori_loop(1, NZ, finish, 0)

def settle(back, w, group_in, mixed_out, g_out, u_out, d_out, mixed, out_sem, mixed_sem):
    outs = (g_out, u_out, d_out)
    writes = [
        pltpu.make_async_copy(
            w.at[m, xb], outs[m].at[:, :, :, pl.ds(LANE * xb, LANE)], out_sem.at[m, xb]
        )
        for m in range(3)
        for xb in range(NX)
    ]
    for write in writes:
        write.start()
    placing = placing_of(group_in[...])
    lasts = []
    for nb in range(4):
        cols = pl.ds(512 * nb, 512)
        mixed[:, cols] = lax.dot_general(
            placing, back[:, cols], (((0,), (0,)), ((), ())), preferred_element_type=F32
        ).astype(BF)
        last = pltpu.make_async_copy(mixed.at[:, cols], mixed_out.at[:, cols], mixed_sem.at[nb])
        last.start()
        lasts.append(last)
    for copy in writes + lasts:
        copy.wait()


def exchange(tokens, group, fine, route, gain, gate, up, down):
    hbm = pl.BlockSpec(memory_space=pltpu.HBM)
    vmem = pl.BlockSpec(memory_space=pltpu.VMEM)
    ready = jax.ShapeDtypeStruct((32, 2, 32, 512), BF)
    dma = pltpu.SemaphoreType.DMA
    count = NZ * ROWS
    scratch = [
        pltpu.VMEM((count, D), BF),
        pltpu.VMEM((3, 32, 64, 64), F32),
        pltpu.VMEM((count, D), BF),
        pltpu.VMEM((NZ, ROWS, D), BF),
        pltpu.VMEM((2, 32, 3, 32, 64), BF),
        pltpu.VMEM((FINE, 2, 1, LANE), F32),
        pltpu.VMEM((NZ, NY, 1, LANE), F32),
        pltpu.VMEM((NZ, NY, ROWS, D), BF),
        pltpu.VMEM((NZ, NY, ROWS, D), BF),
        pltpu.VMEM((NZ, 2, HALF, D), BF),
        pltpu.VMEM((NZ, 2, ROWS, D), BF),
        pltpu.VMEM((NZ, ROWS, D), BF),
        pltpu.VMEM((32, 3, 32, LANE), BF),
        pltpu.VMEM((32, 3, 32, 64), BF),
        dma((4,)),
        dma((NZ, 4)), dma((NZ, 4)),
        dma((NZ,)), dma((NZ,)),
        dma((NZ, 4)), dma((NZ, 4)),
        dma((NZ, 4)), dma((NZ, 4)),
        dma((NZ, 4)), dma((NZ, 4)),
        dma((NZ,)), dma((NZ,)),
        dma, dma,
        dma((NZ, 4)), dma((NZ, 4)),
        dma((NZ,)), dma((NZ,)),
    ]
    back, w = pl.pallas_call(
        kernel,
        out_shape=(
            pltpu.VMEM((NZ, ROWS, D), BF),
            pltpu.VMEM((3, NX, 32, 2, 32, LANE), BF),
        ),
        in_specs=[hbm, vmem, vmem, vmem, vmem, hbm, hbm, hbm],
        out_specs=(vmem, vmem),
        scratch_shapes=scratch,
        compiler_params=pltpu.CompilerParams(
            collective_id=0, has_side_effects=True, vmem_limit_bytes=56 * 1024 * 1024
        ),
    )(tokens, group, fine, route, gain, gate, up, down)
    return pl.pallas_call(
        settle,
        out_shape=(jax.ShapeDtypeStruct((count, D), BF), ready, ready, ready),
        in_specs=[vmem, vmem, vmem],
        out_specs=(hbm,) * 4,
        scratch_shapes=[pltpu.VMEM((count, D), BF), dma((3, NX)), dma((4,))],
        compiler_params=pltpu.CompilerParams(vmem_limit_bytes=16 * 1024 * 1024),
    )(back.reshape(count, D), w, group)


def local(
    tokens, expert_group, expert_fine, route_weight, norm_gain, gate_master, up_master, down_master
):
    mixed, gate, up, down = exchange(
        tokens,
        expert_group.reshape(1, -1),
        expert_fine.T,
        route_weight.T,
        norm_gain.reshape(1, -1),
        gate_master,
        up_master,
        down_master,
    )
    return (mixed,) + tuple(r.reshape(1, D, 512) for r in (gate, up, down))


def solution(mesh):
    fine = Mesh(mesh.devices.reshape(NZ, NY, NX, 2), ("z", "y", "x", "c"))
    fs, tp = ("z", "y"), ("x", "c")
    token = fs + tp
    in_specs = (
        P(token, None),
        P(token),
        P(token, None),
        P(token, None),
        P(fs),
        P(None, fs, tp),
        P(None, fs, tp),
        P(None, fs, tp),
    )
    out_specs = (
        P(token, None),
        P(fs, None, None),
        P(fs, None, None),
        P(fs, None, None),
    )
    return jax.shard_map(local, mesh=fine, in_specs=in_specs, out_specs=out_specs, check_vma=False)
```

```python
import jax
import jax.numpy as jnp
from jax import lax
from jax.experimental import pallas as pl
from jax.experimental.pallas import tpu as pltpu
from jax.sharding import Mesh, PartitionSpec as P

FINE = 4
EPS = 1e-06
BF = jnp.bfloat16
F32 = jnp.float32
NZ, NY, NX = 8, 4, 4
ROWS = 32
HALF = 16
PAIRED = 4
SENT = ("zt", "wt0", "wt", "ws0", "ws", "ag", "pg", "sw", "xw", "xv", "cw", "cv", "rs", "pr", "zb", "pair")
D = 2048
LANE = 128
MESH = pl.DeviceIdType.MESH


def offset_of(s):
    far = (s + 1) // 2
    odd = s % 2
    return (odd * far + (1 - odd) * (NZ - far)) % NZ


def placing_of(group):
    count = NZ * ROWS
    lane = lax.broadcasted_iota(jnp.int32, (count, count), 1)
    sub = lax.broadcasted_iota(jnp.int32, (count, count), 0)
    same = lax.broadcasted_iota(jnp.int32, (16, count), 0) == group
    same = jnp.where(same, 1.0, 0.0)
    earlier = jnp.where(sub < lane, 1.0, 0.0).astype(BF)
    before = jnp.dot(same.astype(BF), earlier, preferred_element_type=F32)
    position = jnp.sum(before * same, axis=0, keepdims=True)
    slot = group.astype(F32) * ROWS + position
    return jnp.where(sub.astype(F32) == slot, 1.0, 0.0).astype(BF)


def kernel(
    tokens_in, group_hbm, fine_hbm, route_hbm, gain_hbm, gate_in, up_in, down_in,
    back, w,
    group_in, fine_in, route_in, gain_in, tok, masters, normed, rows_in, pieces, scales, near,
    a, o, h, f, zsum, wsend, other, w2, acc,
    load_sem, sent, pair_r, cw_r, cv_r, zb_r, zt_r, wt_r, ws_r, sw_r, pg_r, pr_r,
    h_r, f_r, ag_r, xw_r, xv_r,
):
    z, y, x, c = (lax.axis_index(n) for n in ("z", "y", "x", "c"))
    yp, ym = (y + 1) % NY, (y + NY - 1) % NY
    sibling, partner = y + 1 - 2 * (y % 2), NY - 1 - y
    xp, xm = (x + 1) % NX, (x + NX - 1) % NX

    def remote(src, dst, ss, rs, where):
        return pltpu.make_async_remote_copy(
            src_ref=src, dst_ref=dst, send_sem=ss, recv_sem=rs,
            device_id=where, device_id_type=MESH,
        )

    def sem_of(name):
        return sent.at[SENT.index(name)]

    def arrived(ref, sem):
        remote(ref, ref, sem, sem, {"c": 1 - c}).wait_recv()

    def all_sent(ref, name):
        remote(ref, ref, sem_of(name), sem_of(name), {"c": 1 - c}).wait_send()

    def to_z(s):
        return (z + offset_of(s)) % NZ

    def from_z(s):
        return (z + NZ - offset_of(s)) % NZ

    def zt(k):
        t = to_z(k)
        return remote(rows_in.at[t], a.at[k, 0], sem_of("zt"), zt_r.at[k], {"z": t})

    def ws(s, k, name="ws"):
        tz, ty = to_z(s), (y + k) % NY
        return remote(
            wsend.at[FINE * tz + ty], w.at[:, x, NY * z + y, c],
            sem_of(name), ws_r.at[s], {"z": tz, "y": ty},
        )

    def wt(k, j, name="wt"):
        tz, ty = to_z(k), (y + j) % NY
        return remote(
            scales.at[tz // 4, ty // 2], near.at[k, j], sem_of(name), wt_r.at[k],
            {"z": tz, "y": ty},
        )

    def ag(s, j):
        if j == 0:
            src, dst, where = a.at[s, 0], a.at[s, 1], yp
        elif j == 1:
            src, dst, where = a.at[s, 0], a.at[s, 3], ym
        elif j == 2:
            src, dst, where = a.at[s, 1, pl.ds(0, HALF)], a.at[s, 2, pl.ds(0, HALF)], yp
        else:
            src, dst, where = a.at[s, 3, pl.ds(HALF, HALF)], a.at[s, 2, pl.ds(HALF, HALF)], ym
        return remote(src, dst, sem_of("ag"), ag_r.at[s, min(j, 2)], {"y": where})

    def sw(s):
        rows = pl.ds(NY * from_z(s), NY)
        return remote(
            w.at[:, x, rows, c], w2.at[:, x, rows, c], sem_of("sw"), sw_r.at[s], {"y": sibling}
        )

    def gather_x(buf, name, rr, s, j):
        base = NY * from_z(s)
        if j == 0:
            part, where = buf.at[:, x, pl.ds(base, NY), c], xp
        elif j == 1:
            part, where = buf.at[:, x, pl.ds(base, NY), c], xm
        elif j == 2:
            part, where = buf.at[:, xm, pl.ds(base, 2), c], xp
        else:
            part, where = buf.at[:, xp, pl.ds(base + 2, 2), c], xm
        return remote(part, part, sem_of(name), rr.at[s, min(j, 2)], {"x": where})

    def xw(s, j):
        return gather_x(w, "xw", xw_r, s, j)

    def xv(s, j):
        return gather_x(w2, "xv", xv_r, s, j)

    def far_column(buf, s):
        return buf.at[:, (x + 2) % NX, pl.ds(NY * from_z(s), NY), c]

    def cw(s):
        part = w.at[:, :, pl.ds(NY * from_z(s), NY), c]
        return remote(part, part, sem_of("cw"), cw_r, {"c": 1 - c})

    def cv(s):
        part = w2.at[:, :, pl.ds(NY * from_z(s), NY), c]
        return remote(part, part, sem_of("cv"), cv_r, {"c": 1 - c})

    def pg(k):
        src = rows_in.at[z] if isinstance(k, int) and k == 0 else a.at[k, 0]
        return remote(src, a.at[k, 1], sem_of("pg"), pg_r.at[k], {"y": partner})

    def pr(k):
        return remote(o.at[k, 1], f.at[k, 0], sem_of("pr"), pr_r.at[k], {"y": partner})

    def rs(s, j):
        if j == 0:
            src, dst, rr, where = o.at[s, 2, pl.ds(0, HALF)], h.at[s, 0], h_r, ym
        elif j == 1:
            src, dst, rr, where = o.at[s, 2, pl.ds(HALF, HALF)], h.at[s, 1], h_r, yp
        elif j == 2:
            src, dst, rr, where = o.at[s, 1], f.at[s, 0], f_r, ym
        else:
            src, dst, rr, where = o.at[s, 3], f.at[s, 1], f_r, yp
        return remote(src, dst, sem_of("rs"), rr.at[s], {"y": where})

    def zb(s):
        return remote(zsum.at[s], back.at[z], sem_of("zb"), zb_r, {"z": from_z(s)})

    def w_b(s):
        if isinstance(s, int) and s == 0:
            arrived(wsend.at[pl.ds(0, NY - 1)], ws_r.at[s])
        else:
            arrived(wsend.at[pl.ds(0, NY)], ws_r.at[s])
        xw(s, 0).start()
        xw(s, 1).start()
        sw(s).start()

    def w_c(s):
        xw(s, 0).wait_recv()
        xw(s, 2).start()
        xw(s, 1).wait_recv()
        xw(s, 3).start()

    def w_d(s):
        arrived(far_column(w, s), xw_r.at[s, 2])
        cw(s).start()

    def v_b(s):
        sw(s).wait_recv()
        xv(s, 0).start()
        xv(s, 1).start()

    def v_c(s):
        xv(s, 0).wait_recv()
        xv(s, 2).start()
        xv(s, 1).wait_recv()
        xv(s, 3).start()

    def v_d(s):
        arrived(far_column(w2, s), xv_r.at[s, 2])
        cv(s).start()

    def t_a(s):
        zt(s).wait_recv()
        ag(s, 0).start()
        ag(s, 1).start()

    def p_a(k):
        if k > 0:
            zt(k).wait_recv()
        pg(k).start()

    def t_b(s):
        ag(s, 0).wait_recv()
        ag(s, 2).start()
        ag(s, 1).wait_recv()
        ag(s, 3).start()

    def scale_of(s, sources, which):
        lane = lax.broadcasted_iota(jnp.int32, (ROWS, LANE), 1)
        row = lax.broadcasted_iota(jnp.int32, (ROWS, LANE), 0)
        mine = lane == row + ROWS * (z % 4)
        return jnp.concatenate(
            [
                jnp.sum(jnp.where(mine, near[s, j, which], 0.0), axis=1, keepdims=True)
                for j in sources
            ],
            axis=0,
        )

    def expert(s, sources, buf, which, take):
        count = len(sources)
        data = a[s, 0:count].reshape(count * ROWS, D)
        parts = []
        for xb in range(NX):
            both = jnp.concatenate(
                [buf[0, xb].reshape(D, LANE), buf[1, xb].reshape(D, LANE)], axis=1
            )
            r = jnp.dot(data, both, preferred_element_type=F32)
            g, u = r[:, :LANE], r[:, LANE:]
            parts.append((g / (1.0 + jnp.exp(-g)) * u).astype(BF))
        act = jnp.concatenate(parts, axis=1)
        scale = scale_of(s, sources, which)
        for nb in range(8):
            rhs = jnp.concatenate(
                [buf[2, xb, 4 * nb : 4 * nb + 4].reshape(256, LANE) for xb in range(NX)],
                axis=1,
            )
            r = lax.dot_general(act, rhs, (((1,), (1,)), ((), ())), preferred_element_type=F32)
            take(slice(256 * nb, 256 * nb + 256), r.astype(BF).astype(F32) * scale)

    def await_scales(s):
        if isinstance(s, int):
            near_s = near.at[s, pl.ds(1, NY - 1)] if s == 0 else near.at[s]
            arrived(near_s, wt_r.at[s])
        else:
            pl.when(s == 0)(lambda: arrived(near.at[0, pl.ds(1, NY - 1)], wt_r.at[0]))
            pl.when(s > 0)(lambda: arrived(near.at[s], wt_r.at[s]))

    def t_c(s):
        arrived(near.at[s], wt_r.at[s])
        arrived(a.at[s, 2], ag_r.at[s, 2])

        def take(cols, r):
            o[s, :, :, cols] = r.astype(BF).reshape(NY, ROWS, 256)

        expert(s, range(NY), w, y % 2, take)
        rs(s, 0).start()
        rs(s, 1).start()

    pair_sources = (0, 1 + 2 * (y % 2))

    def p_b(k):
        await_scales(k)
        pg(k).wait_recv()

        def take(cols, r):
            acc[k, :, cols] = r

        expert(k, pair_sources, w, y % 2, take)

    def p_c(k):
        def take(cols, r):
            o[k, 0:2, :, cols] = (acc[k, :, cols] + r).astype(BF).reshape(2, ROWS, 256)

        expert(k, pair_sources, w2, 1 - y % 2, take)
        pr(k).start()

    def p_e(k):
        pr(k).wait_recv()
        zsum[k] = (o[k, 0].astype(F32) + f[k, 0].astype(F32)).astype(BF)
        pl.when(k > 0)(lambda: zb(k).start())

    def t_d(s):
        arrived(h.at[s], h_r.at[s])
        o[s, 1, 0:HALF] = (o[s, 1, 0:HALF].astype(F32) + h[s, 0].astype(F32)).astype(BF)
        rs(s, 2).start()
        o[s, 3, HALF:ROWS] = (o[s, 3, HALF:ROWS].astype(F32) + h[s, 1].astype(F32)).astype(BF)
        rs(s, 3).start()

    def t_e(s):
        arrived(f.at[s], f_r.at[s])
        zsum[s] = (
            o[s, 0].astype(F32) + f[s, 0].astype(F32) + f[s, 1].astype(F32)
        ).astype(BF)
        zb(s).start()

    loads = [
        pltpu.make_async_copy(src, dst, load_sem.at[k])
        for k, (src, dst) in enumerate(
            (
                (gain_hbm, gain_in),
                (gate_in, masters.at[0]),
                (up_in, masters.at[1]),
                (down_in, masters.at[2]),
                (tokens_in, tok),
                (group_hbm, group_in),
                (fine_hbm, fine_in),
                (route_hbm, route_in),
            )
        )
    ]
    for load in loads:
        load.start()
    barrier = pltpu.get_barrier_semaphore()
    peers = [{"x": (x + k) % NX} for k in range(1, NX)] + [{"c": 1 - c}]
    for peer in peers:
        pl.semaphore_signal(barrier, inc=1, device_id=peer, device_id_type=MESH)

    def greet(q, carry):
        peer = {"z": (z + q // NY) % NZ, "y": (y + q % NY) % NY}
        pl.semaphore_signal(barrier, inc=1, device_id=peer, device_id_type=MESH)
        return carry

    lax.fori_loop(1, NZ * NY, greet, 0)

    pair = remote(pieces.at[1 - c], other, sem_of("pair"), pair_r, {"c": 1 - c})

    for load in loads[:4]:
        load.wait()
    eye = lax.broadcasted_iota(jnp.int32, (64, 64), 0) == lax.broadcasted_iota(
        jnp.int32, (64, 64), 1
    )
    gain = jnp.sum(jnp.where(eye, gain_in[...], 0.0), axis=1, keepdims=True)

    def cast(e, carry):
        for m in range(3):
            value = masters[m, e] if m == 2 else gain * masters[m, e]
            value = value.astype(BF)
            pieces[0, e, m] = value[:32]
            pieces[1, e, m] = value[32:]
        return carry

    with jax.named_scope("cast"):
        lax.fori_loop(0, NZ * FINE, cast, 0, unroll=4)
    with jax.named_scope("barrier"):
        pl.semaphore_wait(barrier, NZ * NY - 1 + len(peers))
    pair.start()

    for load in loads[4:]:
        load.wait()

    def norm(r, carry):
        wide = tok[pl.ds(pl.multiple_of(r * ROWS, ROWS), ROWS), :].astype(F32)
        mean = jnp.sum(wide * wide, axis=1, keepdims=True) * (1.0 / D)
        normed[pl.ds(pl.multiple_of(r * ROWS, ROWS), ROWS), :] = (
            wide * lax.rsqrt(mean + EPS)
        ).astype(BF)
        return carry

    with jax.named_scope("norm"):
        lax.fori_loop(0, NZ, norm, 0)
        count = NZ * ROWS
        placing = placing_of(group_in[...])
        entry = lax.broadcasted_iota(jnp.int32, (8, count), 0)
        fine_id = entry % FINE
        weight = jnp.where(fine_in[0:1] == fine_id, route_in[0:1], 0.0) + jnp.where(
            fine_in[1:2] == fine_id, route_in[1:2], 0.0
        )
        top = weight.astype(BF).astype(F32)
        weight = jnp.where(entry < FINE, top, weight - top)
        weight = jnp.concatenate([weight, jnp.zeros((8, count), F32)], axis=0).astype(BF)
        sorted_weight = lax.dot_general(
            weight, placing, (((1,), (1,)), ((), ())), preferred_element_type=F32
        )
        sorted_weight = sorted_weight[0:FINE] + sorted_weight[FINE : 2 * FINE]
        for e in range(FINE):
            for p in range(2):
                scales[p, e // 2, e % 2] = sorted_weight[e : e + 1, LANE * p : LANE * p + LANE]
        for nb in range(8):
            part = jnp.dot(
                placing, normed[:, 256 * nb : 256 * nb + 256], preferred_element_type=F32
            )
            rows_in[:, :, 256 * nb : 256 * nb + 256] = part.astype(BF).reshape(NZ, ROWS, 256)

    with jax.named_scope("pair"):
        pair.wait_recv()

    def join(e, carry):
        mine, theirs = pieces[c, e], other[e]
        low = jnp.where(c == 0, mine, theirs)
        high = jnp.where(c == 0, theirs, mine)
        wsend[e] = jnp.concatenate([low, high], axis=-1)
        return carry

    with jax.named_scope("join"):
        lax.fori_loop(0, NZ * FINE, join, 0, unroll=4)

    def send(copy, first, last):
        def one(s, carry):
            copy(s)
            return carry

        lax.fori_loop(first, last, one, 0)

    def send_w(s):
        for k in (1, 3, 2, 0):
            ws(s, k).start()

    def send_t(k):
        zt(k).start()
        for j in range(NY):
            wt(k, j).start()

    for k in (1, 3, 2):
        ws(0, k, "ws0").start()
    w[:, x, NY * z + y, c] = wsend[FINE * z + y]
    send(send_w, 1, 3)
    send(send_t, 1, 3)
    p_a(0)
    send(send_w, 3, NZ)
    send(send_t, 3, NZ)
    for j in range(1, NY):
        wt(0, j, "wt0").start()
    near[0, 0] = scales[z // 4, y // 2]
    a[0, 0] = rows_in[z]

    def run(fn, s):
        with jax.named_scope(fn.__name__):
            fn(s)

    def at(i, when, *todo):
        @pl.when(i == when)
        def _():
            for fn, s in todo:
                run(fn, s)

    run(w_b, 0)
    run(w_b, 1)
    run(p_a, 1)
    run(p_a, 2)

    def w_loop(i, carry):
        pl.when(i < NZ - 2)(lambda: run(w_b, i + 2))
        pl.when(i < NZ)(lambda: run(w_c, i))
        pl.when(i >= 2)(lambda: run(w_d, i - 2))
        at(i, 5, (t_a, 4), (p_a, 3))
        at(i, 6, (v_b, 0))
        at(i, 7, (v_b, 1))
        at(i, 8, (v_b, 2), (t_b, 4))
        at(i, 9, (t_a, 5), (t_a, 6))
        return carry

    lax.fori_loop(0, NZ + 2, w_loop, 0)

    with jax.named_scope("w_end"):
        arrived(w.at[:, :, :, 0], cw_r)
    def v_start(s, carry):
        v_b(s)
        return carry

    def t_loop(i, carry):
        run(t_c, i + PAIRED)

        @pl.when(i == 0)
        def _():
            lax.fori_loop(3, NZ, v_start, 0)

        at(i, 0, (v_c, 0), (v_c, 1))
        run(p_b, (i + 1) % PAIRED)
        at(i, 0, (t_b, 5), (v_c, 2), (t_b, 6), (t_a, 7), (t_d, 4), (v_c, 3))
        at(i, 1, (v_c, 4))
        at(i, 2, (v_c, 5), (t_b, 7), (t_e, 4), (v_c, 6), (t_d, 5), (v_d, 0), (v_d, 1), (t_d, 6))
        at(
            i, 3, (v_c, 7), (v_d, 2), (t_e, 5), (v_d, 3), (v_d, 4), (t_e, 6), (v_d, 5),
            (t_d, 7), (v_d, 6), (v_d, 7),
        )
        return carry

    lax.fori_loop(0, NZ - PAIRED, t_loop, 0)
    with jax.named_scope("v_end"):
        arrived(w2.at[:, :, :, 0], cv_r)

    def p_at(i):
        return i % 3 + 3 * ((3 - i) // 3)

    def p_loop(i, carry):
        run(p_c, p_at(i))
        at(i, 1, (t_e, 7))
        pl.when(i >= 1)(lambda: run(p_e, p_at(i - 1)))
        return carry

    lax.fori_loop(0, PAIRED, p_loop, 0)
    run(p_e, 0)
    back[z] = zsum[0]
    many = NZ - 1
    all_sent(pieces.at[0], "pair")
    all_sent(rows_in.at[pl.ds(0, many)], "zt")
    all_sent(near.at[0, pl.ds(0, NY - 1)], "wt0")
    all_sent(near.at[pl.ds(0, many)], "wt")
    all_sent(wsend.at[pl.ds(0, NY - 1)], "ws0")
    all_sent(wsend.at[pl.ds(0, many * NY)], "ws")
    all_sent(wsend, "sw")
    all_sent(w.at[:, pl.ds(0, 3), :, 0], "xw")
    all_sent(w2.at[:, pl.ds(0, 3), :, 0], "xv")
    all_sent(w.at[:, :, :, 0], "cw")
    all_sent(w2.at[:, :, :, 0], "cv")
    all_sent(a.at[pl.ds(PAIRED, NZ - PAIRED), pl.ds(0, 3)], "ag")
    all_sent(o.at[pl.ds(PAIRED, NZ - PAIRED), pl.ds(0, 3)], "rs")
    all_sent(a.at[pl.ds(0, PAIRED), 0], "pg")
    all_sent(o.at[pl.ds(0, PAIRED), 0], "pr")
    with jax.named_scope("finish"):
        arrived(back.at[pl.ds(0, many)], zb_r)
    all_sent(back.at[pl.ds(0, many)], "zb")


def settle(back, w, group_in, mixed_out, g_out, u_out, d_out, mixed, out_sem, mixed_sem):
    outs = (g_out, u_out, d_out)
    writes = [
        pltpu.make_async_copy(
            w.at[m, xb], outs[m].at[:, :, :, pl.ds(LANE * xb, LANE)], out_sem.at[m, xb]
        )
        for m in range(3)
        for xb in range(NX)
    ]
    for write in writes:
        write.start()
    placing = placing_of(group_in[...])
    lasts = []
    for nb in range(4):
        cols = pl.ds(512 * nb, 512)
        mixed[:, cols] = lax.dot_general(
            placing, back[:, cols], (((0,), (0,)), ((), ())), preferred_element_type=F32
        ).astype(BF)
        last = pltpu.make_async_copy(mixed.at[:, cols], mixed_out.at[:, cols], mixed_sem.at[nb])
        last.start()
        lasts.append(last)
    for copy in writes + lasts:
        copy.wait()


def exchange(tokens, group, fine, route, gain, gate, up, down):
    hbm = pl.BlockSpec(memory_space=pltpu.HBM)
    vmem = pl.BlockSpec(memory_space=pltpu.VMEM)
    ready = jax.ShapeDtypeStruct((32, 2, 32, 512), BF)
    dma = pltpu.SemaphoreType.DMA
    count = NZ * ROWS
    scratch = [
        pltpu.VMEM((1, count), jnp.int32),
        pltpu.VMEM((2, count), jnp.int32),
        pltpu.VMEM((2, count), F32),
        pltpu.VMEM((1, 64), F32),
        pltpu.VMEM((count, D), BF),
        pltpu.VMEM((3, 32, 64, 64), F32),
        pltpu.VMEM((count, D), BF),
        pltpu.VMEM((NZ, ROWS, D), BF),
        pltpu.VMEM((2, 32, 3, 32, 64), BF),
        pltpu.VMEM((2, 2, 2, 1, LANE), F32),
        pltpu.VMEM((NZ, NY, 2, 1, LANE), F32),
        pltpu.VMEM((NZ, NY, ROWS, D), BF),
        pltpu.VMEM((NZ, NY, ROWS, D), BF),
        pltpu.VMEM((NZ, 2, HALF, D), BF),
        pltpu.VMEM((NZ, 2, ROWS, D), BF),
        pltpu.VMEM((NZ, ROWS, D), BF),
        pltpu.VMEM((32, 3, 32, LANE), BF),
        pltpu.VMEM((32, 3, 32, 64), BF),
        pltpu.VMEM((3, NX, 32, 2, 32, LANE), BF),
        pltpu.VMEM((PAIRED, 2 * ROWS, D), F32),
        dma((8,)), dma((len(SENT),)),
        dma, dma, dma, dma,
        dma((NZ,)), dma((NZ,)), dma((NZ,)), dma((NZ,)),
        dma((PAIRED,)), dma((PAIRED,)),
        dma((NZ,)), dma((NZ,)),
        dma((NZ, 3)), dma((NZ, 3)), dma((NZ, 3)),
    ]
    back, w = pl.pallas_call(
        kernel,
        out_shape=(
            pltpu.VMEM((NZ, ROWS, D), BF),
            pltpu.VMEM((3, NX, 32, 2, 32, LANE), BF),
        ),
        in_specs=[hbm] * 8,
        out_specs=(vmem, vmem),
        scratch_shapes=scratch,
        compiler_params=pltpu.CompilerParams(
            collective_id=0, has_side_effects=True, vmem_limit_bytes=56 * 1024 * 1024
        ),
    )(tokens, group, fine, route, gain, gate, up, down)
    return pl.pallas_call(
        settle,
        out_shape=(jax.ShapeDtypeStruct((count, D), BF), ready, ready, ready),
        in_specs=[vmem, vmem, vmem],
        out_specs=(hbm,) * 4,
        scratch_shapes=[pltpu.VMEM((count, D), BF), dma((3, NX)), dma((4,))],
        compiler_params=pltpu.CompilerParams(vmem_limit_bytes=16 * 1024 * 1024),
    )(back.reshape(count, D), w, group)


def local(
    tokens, expert_group, expert_fine, route_weight, norm_gain, gate_master, up_master, down_master
):
    mixed, gate, up, down = exchange(
        tokens,
        expert_group.reshape(1, -1),
        expert_fine.T,
        route_weight.T,
        norm_gain.reshape(1, -1),
        gate_master,
        up_master,
        down_master,
    )
    return (mixed,) + tuple(r.reshape(1, D, 512) for r in (gate, up, down))


def solution(mesh):
    fine = Mesh(mesh.devices.reshape(NZ, NY, NX, 2), ("z", "y", "x", "c"))
    fs, tp = ("z", "y"), ("x", "c")
    token = fs + tp
    in_specs = (
        P(token, None),
        P(token),
        P(token, None),
        P(token, None),
        P(fs),
        P(None, fs, tp),
        P(None, fs, tp),
        P(None, fs, tp),
    )
    out_specs = (
        P(token, None),
        P(fs, None, None),
        P(fs, None, None),
        P(fs, None, None),
    )
    return jax.shard_map(local, mesh=fine, in_specs=in_specs, out_specs=out_specs, check_vma=False)
```

```python
import jax
import jax.numpy as jnp
from jax import lax
from jax.experimental import pallas as pl
from jax.experimental.pallas import tpu as pltpu
from jax.sharding import Mesh, PartitionSpec as P

FINE = 4
EPS = 1e-06
BF = jnp.bfloat16
F32 = jnp.float32
NZ, NY, NX = 8, 4, 4
ROWS = 32
HALF = 16
PAIRED = 4
SENT = ("zt", "wt0", "wt", "ws0", "ws", "ag", "pg", "sw", "xw", "xv", "cw", "cv", "rs", "pr", "zb", "pair")
D = 2048
LANE = 128
MESH = pl.DeviceIdType.MESH


def offset_of(s):
    far = (s + 1) // 2
    odd = s % 2
    return (odd * far + (1 - odd) * (NZ - far)) % NZ


def placing_of(group):
    count = NZ * ROWS
    lane = lax.broadcasted_iota(jnp.int32, (count, count), 1)
    sub = lax.broadcasted_iota(jnp.int32, (count, count), 0)
    same = lax.broadcasted_iota(jnp.int32, (16, count), 0) == group
    same = jnp.where(same, 1.0, 0.0)
    earlier = jnp.where(sub < lane, 1.0, 0.0).astype(BF)
    before = jnp.dot(same.astype(BF), earlier, preferred_element_type=F32)
    position = jnp.sum(before * same, axis=0, keepdims=True)
    slot = group.astype(F32) * ROWS + position
    return jnp.where(sub.astype(F32) == slot, 1.0, 0.0).astype(BF)


def kernel(
    tokens_in, group_hbm, fine_hbm, route_hbm, gain_hbm, gate_in, up_in, down_in,
    back, w,
    group_in, fine_in, route_in, gain_in, tok, masters, normed, rows_in, pieces, scales, near,
    a, o, h, f, zsum, wsend, other, w2, acc,
    load_sem, sent, pair_r, cw_r, cv_r, zb_r, zt_r, wt_r, ws_r, sw_r, pg_r, pr_r,
    h_r, f_r, ag_r, xw_r, xv_r,
):
    z, y, x, c = (lax.axis_index(n) for n in ("z", "y", "x", "c"))
    yp, ym = (y + 1) % NY, (y + NY - 1) % NY
    sibling, partner = y + 1 - 2 * (y % 2), NY - 1 - y
    xp, xm = (x + 1) % NX, (x + NX - 1) % NX

    def remote(src, dst, ss, rs, where):
        return pltpu.make_async_remote_copy(
            src_ref=src, dst_ref=dst, send_sem=ss, recv_sem=rs,
            device_id=where, device_id_type=MESH,
        )

    def sem_of(name):
        return sent.at[SENT.index(name)]

    def arrived(ref, sem):
        remote(ref, ref, sem, sem, {"c": 1 - c}).wait_recv()

    def all_sent(ref, name):
        remote(ref, ref, sem_of(name), sem_of(name), {"c": 1 - c}).wait_send()

    def to_z(s):
        return (z + offset_of(s)) % NZ

    def from_z(s):
        return (z + NZ - offset_of(s)) % NZ

    def zt(k):
        t = to_z(k)
        return remote(rows_in.at[t], a.at[k, 0], sem_of("zt"), zt_r.at[k], {"z": t})

    def ws(s, k, name="ws"):
        tz, ty = to_z(s), (y + k) % NY
        return remote(
            wsend.at[FINE * tz + ty], w.at[:, x, NY * z + y, c],
            sem_of(name), ws_r.at[s], {"z": tz, "y": ty},
        )

    def wt(k, j, name="wt"):
        tz, ty = to_z(k), (y + j) % NY
        return remote(
            scales.at[tz // 4, ty // 2], near.at[k, j], sem_of(name), wt_r.at[k],
            {"z": tz, "y": ty},
        )

    def ag(s, j):
        if j == 0:
            src, dst, where = a.at[s, 0], a.at[s, 1], yp
        elif j == 1:
            src, dst, where = a.at[s, 0], a.at[s, 3], ym
        elif j == 2:
            src, dst, where = a.at[s, 1, pl.ds(0, HALF)], a.at[s, 2, pl.ds(0, HALF)], yp
        else:
            src, dst, where = a.at[s, 3, pl.ds(HALF, HALF)], a.at[s, 2, pl.ds(HALF, HALF)], ym
        return remote(src, dst, sem_of("ag"), ag_r.at[s, min(j, 2)], {"y": where})

    def sw(s):
        rows = pl.ds(NY * from_z(s), NY)
        return remote(
            w.at[:, x, rows, c], w2.at[:, x, rows, c], sem_of("sw"), sw_r.at[s], {"y": sibling}
        )

    def gather_x(buf, name, rr, s, j):
        base = NY * from_z(s)
        if j == 0:
            part, where = buf.at[:, x, pl.ds(base, NY), c], xp
        elif j == 1:
            part, where = buf.at[:, x, pl.ds(base, NY), c], xm
        elif j == 2:
            part, where = buf.at[:, xm, pl.ds(base, 2), c], xp
        else:
            part, where = buf.at[:, xp, pl.ds(base + 2, 2), c], xm
        return remote(part, part, sem_of(name), rr.at[s, min(j, 2)], {"x": where})

    def xw(s, j):
        return gather_x(w, "xw", xw_r, s, j)

    def xv(s, j):
        return gather_x(w2, "xv", xv_r, s, j)

    def far_column(buf, s):
        return buf.at[:, (x + 2) % NX, pl.ds(NY * from_z(s), NY), c]

    def cw(s):
        part = w.at[:, :, pl.ds(NY * from_z(s), NY), c]
        return remote(part, part, sem_of("cw"), cw_r, {"c": 1 - c})

    def cv(s):
        part = w2.at[:, :, pl.ds(NY * from_z(s), NY), c]
        return remote(part, part, sem_of("cv"), cv_r, {"c": 1 - c})

    def pg(k):
        src = rows_in.at[z] if isinstance(k, int) and k == 0 else a.at[k, 0]
        return remote(src, a.at[k, 1], sem_of("pg"), pg_r.at[k], {"y": partner})

    def pr(k):
        return remote(o.at[k, 1], f.at[k, 0], sem_of("pr"), pr_r.at[k], {"y": partner})

    def rs(s, j):
        if j == 0:
            src, dst, rr, where = o.at[s, 2, pl.ds(0, HALF)], h.at[s, 0], h_r, ym
        elif j == 1:
            src, dst, rr, where = o.at[s, 2, pl.ds(HALF, HALF)], h.at[s, 1], h_r, yp
        elif j == 2:
            src, dst, rr, where = o.at[s, 1], f.at[s, 0], f_r, ym
        else:
            src, dst, rr, where = o.at[s, 3], f.at[s, 1], f_r, yp
        return remote(src, dst, sem_of("rs"), rr.at[s], {"y": where})

    def zb(s):
        return remote(zsum.at[s], back.at[z], sem_of("zb"), zb_r, {"z": from_z(s)})

    def w_b(s):
        if isinstance(s, int) and s == 0:
            arrived(wsend.at[pl.ds(0, NY - 1)], ws_r.at[s])
        else:
            arrived(wsend.at[pl.ds(0, NY)], ws_r.at[s])
        xw(s, 0).start()
        xw(s, 1).start()
        sw(s).start()

    def w_c(s):
        xw(s, 0).wait_recv()
        xw(s, 2).start()
        xw(s, 1).wait_recv()
        xw(s, 3).start()

    def w_d(s):
        arrived(far_column(w, s), xw_r.at[s, 2])
        cw(s).start()

    def v_b(s):
        sw(s).wait_recv()
        xv(s, 0).start()
        xv(s, 1).start()

    def v_c(s):
        xv(s, 0).wait_recv()
        xv(s, 2).start()
        xv(s, 1).wait_recv()
        xv(s, 3).start()

    def v_d(s):
        arrived(far_column(w2, s), xv_r.at[s, 2])
        cv(s).start()

    def t_a(s):
        zt(s).wait_recv()
        ag(s, 0).start()
        ag(s, 1).start()

    def p_a(k):
        if k > 0:
            zt(k).wait_recv()
        pg(k).start()

    def t_b(s):
        ag(s, 0).wait_recv()
        ag(s, 2).start()
        ag(s, 1).wait_recv()
        ag(s, 3).start()

    def scale_of(s, sources, which):
        lane = lax.broadcasted_iota(jnp.int32, (ROWS, LANE), 1)
        row = lax.broadcasted_iota(jnp.int32, (ROWS, LANE), 0)
        mine = lane == row + ROWS * (z % 4)
        return jnp.concatenate(
            [
                jnp.sum(jnp.where(mine, near[s, j, which], 0.0), axis=1, keepdims=True)
                for j in sources
            ],
            axis=0,
        )

    def expert(s, sources, buf, which, take):
        count = len(sources)
        data = a[s, 0:count].reshape(count * ROWS, D)
        parts = []
        for xb in range(NX):
            both = jnp.concatenate(
                [buf[0, xb].reshape(D, LANE), buf[1, xb].reshape(D, LANE)], axis=1
            )
            r = jnp.dot(data, both, preferred_element_type=F32)
            g, u = r[:, :LANE], r[:, LANE:]
            parts.append((g / (1.0 + jnp.exp(-g)) * u).astype(BF))
        act = jnp.concatenate(parts, axis=1)
        scale = scale_of(s, sources, which)
        for nb in range(8):
            rhs = jnp.concatenate(
                [buf[2, xb, 4 * nb : 4 * nb + 4].reshape(256, LANE) for xb in range(NX)],
                axis=1,
            )
            r = lax.dot_general(act, rhs, (((1,), (1,)), ((), ())), preferred_element_type=F32)
            take(slice(256 * nb, 256 * nb + 256), r.astype(BF).astype(F32) * scale)

    def await_scales(s):
        if isinstance(s, int):
            near_s = near.at[s, pl.ds(1, NY - 1)] if s == 0 else near.at[s]
            arrived(near_s, wt_r.at[s])
        else:
            pl.when(s == 0)(lambda: arrived(near.at[0, pl.ds(1, NY - 1)], wt_r.at[0]))
            pl.when(s > 0)(lambda: arrived(near.at[s], wt_r.at[s]))

    def t_c(s):
        arrived(near.at[s], wt_r.at[s])
        arrived(a.at[s, 2], ag_r.at[s, 2])

        def take(cols, r):
            o[s, :, :, cols] = r.astype(BF).reshape(NY, ROWS, 256)

        expert(s, range(NY), w, y % 2, take)
        rs(s, 0).start()
        rs(s, 1).start()

    pair_sources = (0, 1 + 2 * (y % 2))

    def p_b(k):
        await_scales(k)
        pg(k).wait_recv()

        def take(cols, r):
            acc[(k + 1) % NZ, :, cols] = r

        expert(k, pair_sources, w, y % 2, take)

    def p_c(k):
        def take(cols, r):
            o[k, 0:2, :, cols] = (acc[(k + 1) % NZ, :, cols] + r).astype(BF).reshape(2, ROWS, 256)

        expert(k, pair_sources, w2, 1 - y % 2, take)
        pr(k).start()

    def p_e(k):
        pr(k).wait_recv()
        zsum[k] = (o[k, 0].astype(F32) + f[k, 0].astype(F32)).astype(BF)
        pl.when(k > 0)(lambda: zb(k).start())

    def t_d(s):
        arrived(h.at[s], h_r.at[s])
        o[s, 1, 0:HALF] = (o[s, 1, 0:HALF].astype(F32) + h[s, 0].astype(F32)).astype(BF)
        rs(s, 2).start()
        o[s, 3, HALF:ROWS] = (o[s, 3, HALF:ROWS].astype(F32) + h[s, 1].astype(F32)).astype(BF)
        rs(s, 3).start()

    def t_e(s):
        arrived(f.at[s], f_r.at[s])
        zsum[s] = (
            o[s, 0].astype(F32) + f[s, 0].astype(F32) + f[s, 1].astype(F32)
        ).astype(BF)
        zb(s).start()

    loads = [
        pltpu.make_async_copy(src, dst, load_sem.at[k])
        for k, (src, dst) in enumerate(
            (
                (gain_hbm, gain_in),
                (gate_in, masters.at[0]),
                (up_in, masters.at[1]),
                (down_in, masters.at[2]),
                (tokens_in, tok),
                (group_hbm, group_in),
                (fine_hbm, fine_in),
                (route_hbm, route_in),
            )
        )
    ]
    for load in loads:
        load.start()
    barrier = pltpu.get_barrier_semaphore()
    peers = [{"x": (x + k) % NX} for k in range(1, NX)] + [{"c": 1 - c}]
    for peer in peers:
        pl.semaphore_signal(barrier, inc=1, device_id=peer, device_id_type=MESH)

    def greet(q, carry):
        peer = {"z": (z + q // NY) % NZ, "y": (y + q % NY) % NY}
        pl.semaphore_signal(barrier, inc=1, device_id=peer, device_id_type=MESH)
        return carry

    lax.fori_loop(1, NZ * NY, greet, 0)

    pair = remote(pieces.at[1 - c], other, sem_of("pair"), pair_r, {"c": 1 - c})

    for load in loads[:4]:
        load.wait()
    eye = lax.broadcasted_iota(jnp.int32, (64, 64), 0) == lax.broadcasted_iota(
        jnp.int32, (64, 64), 1
    )
    gain = jnp.sum(jnp.where(eye, gain_in[...], 0.0), axis=1, keepdims=True)

    def cast(e, carry):
        for m in range(3):
            value = masters[m, e] if m == 2 else gain * masters[m, e]
            value = value.astype(BF)
            pieces[0, e, m] = value[:32]
            pieces[1, e, m] = value[32:]
        return carry

    with jax.named_scope("cast"):
        lax.fori_loop(0, NZ * FINE, cast, 0, unroll=4)
    with jax.named_scope("barrier"):
        pl.semaphore_wait(barrier, NZ * NY - 1 + len(peers))
    pair.start()

    for load in loads[4:]:
        load.wait()

    def norm(r, carry):
        wide = tok[pl.ds(pl.multiple_of(r * ROWS, ROWS), ROWS), :].astype(F32)
        mean = jnp.sum(wide * wide, axis=1, keepdims=True) * (1.0 / D)
        normed[pl.ds(pl.multiple_of(r * ROWS, ROWS), ROWS), :] = (
            wide * lax.rsqrt(mean + EPS)
        ).astype(BF)
        return carry

    with jax.named_scope("norm"):
        lax.fori_loop(0, NZ, norm, 0)
        count = NZ * ROWS
        placing = placing_of(group_in[...])
        entry = lax.broadcasted_iota(jnp.int32, (8, count), 0)
        fine_id = entry % FINE
        weight = jnp.where(fine_in[0:1] == fine_id, route_in[0:1], 0.0) + jnp.where(
            fine_in[1:2] == fine_id, route_in[1:2], 0.0
        )
        top = weight.astype(BF).astype(F32)
        weight = jnp.where(entry < FINE, top, weight - top)
        weight = jnp.concatenate([weight, jnp.zeros((8, count), F32)], axis=0).astype(BF)
        sorted_weight = lax.dot_general(
            weight, placing, (((1,), (1,)), ((), ())), preferred_element_type=F32
        )
        sorted_weight = sorted_weight[0:FINE] + sorted_weight[FINE : 2 * FINE]
        for e in range(FINE):
            for p in range(2):
                scales[p, e // 2, e % 2] = sorted_weight[e : e + 1, LANE * p : LANE * p + LANE]
        for nb in range(8):
            part = jnp.dot(
                placing, normed[:, 256 * nb : 256 * nb + 256], preferred_element_type=F32
            )
            rows_in[:, :, 256 * nb : 256 * nb + 256] = part.astype(BF).reshape(NZ, ROWS, 256)

    with jax.named_scope("pair"):
        pair.wait_recv()

    def join(s):
        for n in range(FINE):
            e = FINE * to_z(s) + n
            mine, theirs = pieces[c, e], other[e]
            low = jnp.where(c == 0, mine, theirs)
            high = jnp.where(c == 0, theirs, mine)
            wsend[e] = jnp.concatenate([low, high], axis=-1)

    def send(copy, first, last):
        def one(s, carry):
            copy(s)
            return carry

        lax.fori_loop(first, last, one, 0)

    def send_w(s):
        join(s)
        for k in (1, 3, 2, 0):
            ws(s, k).start()

    def send_t(k):
        zt(k).start()
        for j in range(NY):
            wt(k, j).start()

    join(0)
    for k in (1, 3, 2):
        ws(0, k, "ws0").start()
    w[:, x, NY * z + y, c] = wsend[FINE * z + y]
    send(send_w, 1, 3)
    send(send_t, 1, 3)
    p_a(0)
    send(send_w, 3, NZ)
    send(send_t, 3, NZ)
    for j in range(1, NY):
        wt(0, j, "wt0").start()
    near[0, 0] = scales[z // 4, y // 2]
    a[0, 0] = rows_in[z]

    def run(fn, s):
        with jax.named_scope(fn.__name__):
            fn(s)

    def at(i, when, *todo):
        @pl.when(i == when)
        def _():
            for fn, s in todo:
                run(fn, s)

    run(w_b, 0)
    run(w_b, 1)
    run(p_a, 1)
    run(p_a, 2)

    def w_loop(i, carry):
        pl.when(i < NZ - 2)(lambda: run(w_b, i + 2))
        pl.when(i < NZ)(lambda: run(w_c, i))
        pl.when(i >= 2)(lambda: run(w_d, i - 2))
        at(i, 5, (t_a, 3), (t_a, 4))
        at(i, 6, (v_b, 0))
        at(i, 7, (v_b, 1), (t_b, 3))
        at(i, 8, (v_b, 2), (v_b, 3), (t_b, 4))
        at(i, 9, (v_b, 4), (t_a, 5), (t_a, 6))
        return carry

    lax.fori_loop(0, NZ + 2, w_loop, 0)

    with jax.named_scope("w_end"):
        arrived(w.at[:, :, :, 0], cw_r)
    def v_start(s, carry):
        v_b(s)
        return carry

    def t_loop(i, carry):
        at(i, 2, (t_d, 4))
        run(t_c, i + 3)

        @pl.when(i == 0)
        def _():
            lax.fori_loop(5, NZ, v_start, 0)

        at(i, 0, (v_c, 0))
        at(i, 1, (v_c, 1))
        at(i, 3, (v_c, 6), (t_e, 3))
        pl.when(i >= 1)(lambda: run(p_b, i % 3))
        at(i, 1, (t_b, 5), (v_c, 2), (t_b, 6), (t_d, 3), (v_c, 3))
        at(i, 2, (v_c, 4), (v_c, 5))
        at(i, 3, (v_c, 7), (t_d, 5), (v_d, 0), (t_e, 4), (t_d, 6), (p_a, 7))
        at(i, 3, *((v_d, k) for k in range(1, NZ)))
        at(i, 3, (t_e, 5))
        return carry

    lax.fori_loop(0, NZ - PAIRED, t_loop, 0)
    with jax.named_scope("v_end"):
        arrived(w2.at[:, :, :, 0], cv_r)

    def p_at(i):
        return (i + 1) % 4 + 4 * ((i // 2) * (3 - i))

    def p_loop(i, carry):
        run(p_c, p_at(i))
        at(i, 0, (t_e, 6))
        at(i, 1, (p_b, 7))
        return carry

    lax.fori_loop(0, PAIRED, p_loop, 0)

    def e_loop(i, carry):
        run(p_e, p_at(i))
        return carry

    lax.fori_loop(0, PAIRED, e_loop, 0)
    back[z] = zsum[0]
    many = NZ - 1
    all_sent(pieces.at[0], "pair")
    all_sent(rows_in.at[pl.ds(0, many)], "zt")
    all_sent(near.at[0, pl.ds(0, NY - 1)], "wt0")
    all_sent(near.at[pl.ds(0, many)], "wt")
    all_sent(wsend.at[pl.ds(0, NY - 1)], "ws0")
    all_sent(wsend.at[pl.ds(0, many * NY)], "ws")
    all_sent(wsend, "sw")
    all_sent(w.at[:, pl.ds(0, 3), :, 0], "xw")
    all_sent(w2.at[:, pl.ds(0, 3), :, 0], "xv")
    all_sent(w.at[:, :, :, 0], "cw")
    all_sent(w2.at[:, :, :, 0], "cv")
    all_sent(a.at[pl.ds(0, NZ - PAIRED), pl.ds(0, 3)], "ag")
    all_sent(o.at[pl.ds(0, NZ - PAIRED), pl.ds(0, 3)], "rs")
    all_sent(a.at[pl.ds(0, PAIRED), 0], "pg")
    all_sent(o.at[pl.ds(0, PAIRED), 0], "pr")
    with jax.named_scope("finish"):
        arrived(back.at[pl.ds(0, many)], zb_r)
    all_sent(back.at[pl.ds(0, many)], "zb")


def settle(back, w, group_in, mixed_out, g_out, u_out, d_out, mixed, out_sem, mixed_sem):
    outs = (g_out, u_out, d_out)
    writes = [
        pltpu.make_async_copy(
            w.at[m, xb], outs[m].at[:, :, :, pl.ds(LANE * xb, LANE)], out_sem.at[m, xb]
        )
        for m in range(3)
        for xb in range(NX)
    ]
    for write in writes:
        write.start()
    placing = placing_of(group_in[...])
    lasts = []
    for nb in range(4):
        cols = pl.ds(512 * nb, 512)
        mixed[:, cols] = lax.dot_general(
            placing, back[:, cols], (((0,), (0,)), ((), ())), preferred_element_type=F32
        ).astype(BF)
        last = pltpu.make_async_copy(mixed.at[:, cols], mixed_out.at[:, cols], mixed_sem.at[nb])
        last.start()
        lasts.append(last)
    for copy in writes + lasts:
        copy.wait()


def exchange(tokens, group, fine, route, gain, gate, up, down):
    hbm = pl.BlockSpec(memory_space=pltpu.HBM)
    vmem = pl.BlockSpec(memory_space=pltpu.VMEM)
    ready = jax.ShapeDtypeStruct((32, 2, 32, 512), BF)
    dma = pltpu.SemaphoreType.DMA
    count = NZ * ROWS
    scratch = [
        pltpu.VMEM((1, count), jnp.int32),
        pltpu.VMEM((2, count), jnp.int32),
        pltpu.VMEM((2, count), F32),
        pltpu.VMEM((1, 64), F32),
        pltpu.VMEM((count, D), BF),
        pltpu.VMEM((3, 32, 64, 64), F32),
        pltpu.VMEM((count, D), BF),
        pltpu.VMEM((NZ, ROWS, D), BF),
        pltpu.VMEM((2, 32, 3, 32, 64), BF),
        pltpu.VMEM((2, 2, 2, 1, LANE), F32),
        pltpu.VMEM((NZ, NY, 2, 1, LANE), F32),
        pltpu.VMEM((NZ, NY, ROWS, D), BF),
        pltpu.VMEM((NZ, NY, ROWS, D), BF),
        pltpu.VMEM((NZ, 2, HALF, D), BF),
        pltpu.VMEM((NZ, 2, ROWS, D), BF),
        pltpu.VMEM((NZ, ROWS, D), BF),
        pltpu.VMEM((32, 3, 32, LANE), BF),
        pltpu.VMEM((32, 3, 32, 64), BF),
        pltpu.VMEM((3, NX, 32, 2, 32, LANE), BF),
        pltpu.VMEM((PAIRED, 2 * ROWS, D), F32),
        dma((8,)), dma((len(SENT),)),
        dma, dma, dma, dma,
        dma((NZ,)), dma((NZ,)), dma((NZ,)), dma((NZ,)),
        dma((NZ,)), dma((NZ,)),
        dma((NZ,)), dma((NZ,)),
        dma((NZ, 3)), dma((NZ, 3)), dma((NZ, 3)),
    ]
    back, w = pl.pallas_call(
        kernel,
        out_shape=(
            pltpu.VMEM((NZ, ROWS, D), BF),
            pltpu.VMEM((3, NX, 32, 2, 32, LANE), BF),
        ),
        in_specs=[hbm] * 8,
        out_specs=(vmem, vmem),
        scratch_shapes=scratch,
        compiler_params=pltpu.CompilerParams(
            collective_id=0, has_side_effects=True, vmem_limit_bytes=56 * 1024 * 1024
        ),
    )(tokens, group, fine, route, gain, gate, up, down)
    return pl.pallas_call(
        settle,
        out_shape=(jax.ShapeDtypeStruct((count, D), BF), ready, ready, ready),
        in_specs=[vmem, vmem, vmem],
        out_specs=(hbm,) * 4,
        scratch_shapes=[pltpu.VMEM((count, D), BF), dma((3, NX)), dma((4,))],
        compiler_params=pltpu.CompilerParams(vmem_limit_bytes=16 * 1024 * 1024),
    )(back.reshape(count, D), w, group)


def local(
    tokens, expert_group, expert_fine, route_weight, norm_gain, gate_master, up_master, down_master
):
    mixed, gate, up, down = exchange(
        tokens,
        expert_group.reshape(1, -1),
        expert_fine.T,
        route_weight.T,
        norm_gain.reshape(1, -1),
        gate_master,
        up_master,
        down_master,
    )
    return (mixed,) + tuple(r.reshape(1, D, 512) for r in (gate, up, down))


def solution(mesh):
    fine = Mesh(mesh.devices.reshape(NZ, NY, NX, 2), ("z", "y", "x", "c"))
    fs, tp = ("z", "y"), ("x", "c")
    token = fs + tp
    in_specs = (
        P(token, None),
        P(token),
        P(token, None),
        P(token, None),
        P(fs),
        P(None, fs, tp),
        P(None, fs, tp),
        P(None, fs, tp),
    )
    out_specs = (
        P(token, None),
        P(fs, None, None),
        P(fs, None, None),
        P(fs, None, None),
    )
    return jax.shard_map(local, mesh=fine, in_specs=in_specs, out_specs=out_specs, check_vma=False)
```

```python
import jax
import jax.numpy as jnp
from jax import lax
from jax.experimental import pallas as pl
from jax.experimental.pallas import tpu as pltpu
from jax.sharding import Mesh, PartitionSpec as P

FINE = 4
EPS = 1e-06
BF = jnp.bfloat16
F32 = jnp.float32
NZ, NY, NX = 8, 4, 4
ROWS = 32
HALF = 16
PAIRED = 4
SENT = ("zt", "wt0", "wt", "ws0", "ws", "ag", "pg", "sw", "xw", "xv", "cw", "cv", "rs", "pr", "zb", "pair")
D = 2048
LANE = 128
MESH = pl.DeviceIdType.MESH


def offset_of(s):
    far = (s + 1) // 2
    odd = s % 2
    return (odd * far + (1 - odd) * (NZ - far)) % NZ


def placing_of(group):
    count = NZ * ROWS
    lane = lax.broadcasted_iota(jnp.int32, (count, count), 1)
    sub = lax.broadcasted_iota(jnp.int32, (count, count), 0)
    same = lax.broadcasted_iota(jnp.int32, (16, count), 0) == group
    same = jnp.where(same, 1.0, 0.0)
    earlier = jnp.where(sub < lane, 1.0, 0.0).astype(BF)
    before = jnp.dot(same.astype(BF), earlier, preferred_element_type=F32)
    position = jnp.sum(before * same, axis=0, keepdims=True)
    slot = group.astype(F32) * ROWS + position
    return jnp.where(sub.astype(F32) == slot, 1.0, 0.0).astype(BF)


def kernel(
    tokens_in, group_hbm, fine_hbm, route_hbm, gain_hbm, gate_in, up_in, down_in,
    back, w,
    group_in, fine_in, route_in, gain_in, tok, masters, normed, rows_in, pieces, scales, near,
    a, o, h, f, zsum, wsend, other, w2, acc,
    load_sem, sent, pair_r, cw_r, cv_r, zb_r, zt_r, wt_r, ws_r, sw_r, pg_r, pr_r,
    h_r, f_r, ag_r, xw_r, xv_r,
):
    z, y, x, c = (lax.axis_index(n) for n in ("z", "y", "x", "c"))
    yp, ym = (y + 1) % NY, (y + NY - 1) % NY
    sibling, partner = y + 1 - 2 * (y % 2), NY - 1 - y
    xp, xm = (x + 1) % NX, (x + NX - 1) % NX

    def remote(src, dst, ss, rs, where):
        return pltpu.make_async_remote_copy(
            src_ref=src, dst_ref=dst, send_sem=ss, recv_sem=rs,
            device_id=where, device_id_type=MESH,
        )

    def sem_of(name):
        return sent.at[SENT.index(name)]

    def arrived(ref, sem):
        remote(ref, ref, sem, sem, {"c": 1 - c}).wait_recv()

    def all_sent(ref, name):
        remote(ref, ref, sem_of(name), sem_of(name), {"c": 1 - c}).wait_send()

    def to_z(s):
        return (z + offset_of(s)) % NZ

    def from_z(s):
        return (z + NZ - offset_of(s)) % NZ

    def zt(k):
        t = to_z(k)
        return remote(rows_in.at[t], a.at[k, 0], sem_of("zt"), zt_r.at[k], {"z": t})

    def ws(s, k, name="ws"):
        tz, ty = to_z(s), (y + k) % NY
        return remote(
            wsend.at[FINE * tz + ty], w.at[:, x, NY * z + y, c],
            sem_of(name), ws_r.at[s], {"z": tz, "y": ty},
        )

    def wt(k, j, name="wt"):
        tz, ty = to_z(k), (y + j) % NY
        return remote(
            scales.at[tz // 4, ty // 2], near.at[k, j], sem_of(name), wt_r.at[k],
            {"z": tz, "y": ty},
        )

    def ag(s, j):
        if j == 0:
            src, dst, where = a.at[s, 0], a.at[s, 1], yp
        elif j == 1:
            src, dst, where = a.at[s, 0], a.at[s, 3], ym
        elif j == 2:
            src, dst, where = a.at[s, 1, pl.ds(0, HALF)], a.at[s, 2, pl.ds(0, HALF)], yp
        else:
            src, dst, where = a.at[s, 3, pl.ds(HALF, HALF)], a.at[s, 2, pl.ds(HALF, HALF)], ym
        return remote(src, dst, sem_of("ag"), ag_r.at[s - 3, min(j, 2)], {"y": where})

    def sw(s):
        rows = pl.ds(NY * from_z(s), NY)
        return remote(
            w.at[:, x, rows, c], w2.at[:, x, rows, c], sem_of("sw"), sw_r.at[s], {"y": sibling}
        )

    def gather_x(buf, name, rr, s, j):
        base = NY * from_z(s)
        if j == 0:
            part, where = buf.at[:, x, pl.ds(base, NY), c], xp
        elif j == 1:
            part, where = buf.at[:, x, pl.ds(base, NY), c], xm
        elif j == 2:
            part, where = buf.at[:, xm, pl.ds(base, 2), c], xp
        else:
            part, where = buf.at[:, xp, pl.ds(base + 2, 2), c], xm
        return remote(part, part, sem_of(name), rr.at[s, min(j, 2)], {"x": where})

    def xw(s, j):
        return gather_x(w, "xw", xw_r, s, j)

    def xv(s, j):
        return gather_x(w2, "xv", xv_r, s, j)

    def far_column(buf, s):
        return buf.at[:, (x + 2) % NX, pl.ds(NY * from_z(s), NY), c]

    def cw(s):
        part = w.at[:, :, pl.ds(NY * from_z(s), NY), c]
        return remote(part, part, sem_of("cw"), cw_r, {"c": 1 - c})

    def cv(s):
        part = w2.at[:, :, pl.ds(NY * from_z(s), NY), c]
        return remote(part, part, sem_of("cv"), cv_r, {"c": 1 - c})

    def pg(k):
        src = rows_in.at[z] if isinstance(k, int) and k == 0 else a.at[k, 0]
        return remote(src, a.at[k, 1], sem_of("pg"), pg_r.at[(k + 1) % NZ], {"y": partner})

    def pr(k):
        return remote(o.at[k, 1], f.at[k, 0], sem_of("pr"), pr_r.at[(k + 1) % NZ], {"y": partner})

    def rs(s, j):
        if j == 0:
            src, dst, rr, where = o.at[s, 2, pl.ds(0, HALF)], h.at[s, 0], h_r, ym
        elif j == 1:
            src, dst, rr, where = o.at[s, 2, pl.ds(HALF, HALF)], h.at[s, 1], h_r, yp
        elif j == 2:
            src, dst, rr, where = o.at[s, 1], f.at[s, 0], f_r, ym
        else:
            src, dst, rr, where = o.at[s, 3], f.at[s, 1], f_r, yp
        return remote(src, dst, sem_of("rs"), rr.at[s - 3], {"y": where})

    def zb(s):
        return remote(zsum.at[s], back.at[z], sem_of("zb"), zb_r, {"z": from_z(s)})

    def w_b(s):
        if isinstance(s, int) and s == 0:
            arrived(wsend.at[pl.ds(0, NY - 1)], ws_r.at[s])
        else:
            arrived(wsend.at[pl.ds(0, NY)], ws_r.at[s])
        xw(s, 0).start()
        xw(s, 1).start()
        sw(s).start()

    def w_c(s):
        xw(s, 0).wait_recv()
        xw(s, 2).start()
        xw(s, 1).wait_recv()
        xw(s, 3).start()

    def w_d(s):
        arrived(far_column(w, s), xw_r.at[s, 2])
        cw(s).start()

    def v_b(s):
        sw(s).wait_recv()
        xv(s, 0).start()
        xv(s, 1).start()

    def v_c(s):
        xv(s, 0).wait_recv()
        xv(s, 2).start()
        xv(s, 1).wait_recv()
        xv(s, 3).start()

    def v_d(s):
        arrived(far_column(w2, s), xv_r.at[s, 2])
        cv(s).start()

    def t_a(s):
        zt(s).wait_recv()
        ag(s, 0).start()
        ag(s, 1).start()

    def p_a(k):
        if k > 0:
            zt(k).wait_recv()
        pg(k).start()

    def t_b(s):
        ag(s, 0).wait_recv()
        ag(s, 2).start()
        ag(s, 1).wait_recv()
        ag(s, 3).start()

    def scale_of(s, sources, which):
        lane = lax.broadcasted_iota(jnp.int32, (ROWS, LANE), 1)
        row = lax.broadcasted_iota(jnp.int32, (ROWS, LANE), 0)
        mine = lane == row + ROWS * (z % 4)
        return jnp.concatenate(
            [
                jnp.sum(jnp.where(mine, near[s, j, which], 0.0), axis=1, keepdims=True)
                for j in sources
            ],
            axis=0,
        )

    def expert(s, sources, buf, which, take):
        count = len(sources)
        data = a[s, 0:count].reshape(count * ROWS, D)
        parts = []
        for xb in range(NX):
            both = jnp.concatenate(
                [buf[0, xb].reshape(D, LANE), buf[1, xb].reshape(D, LANE)], axis=1
            )
            r = jnp.dot(data, both, preferred_element_type=F32)
            g, u = r[:, :LANE], r[:, LANE:]
            parts.append((g / (1.0 + jnp.exp(-g)) * u).astype(BF))
        act = jnp.concatenate(parts, axis=1)
        scale = scale_of(s, sources, which)
        for nb in range(8):
            rhs = jnp.concatenate(
                [buf[2, xb, 4 * nb : 4 * nb + 4].reshape(256, LANE) for xb in range(NX)],
                axis=1,
            )
            r = lax.dot_general(act, rhs, (((1,), (1,)), ((), ())), preferred_element_type=F32)
            take(slice(256 * nb, 256 * nb + 256), r.astype(BF).astype(F32) * scale)

    def await_scales(s):
        if isinstance(s, int):
            near_s = near.at[s, pl.ds(1, NY - 1)] if s == 0 else near.at[s]
            arrived(near_s, wt_r.at[s])
        else:
            pl.when(s == 0)(lambda: arrived(near.at[0, pl.ds(1, NY - 1)], wt_r.at[0]))
            pl.when(s > 0)(lambda: arrived(near.at[s], wt_r.at[s]))

    def t_c(s):
        arrived(near.at[s], wt_r.at[s])
        arrived(a.at[s, 2], ag_r.at[s - 3, 2])

        def take(cols, r):
            o[s, :, :, cols] = r.astype(BF).reshape(NY, ROWS, 256)

        expert(s, range(NY), w, y % 2, take)
        rs(s, 0).start()
        rs(s, 1).start()

    pair_sources = (0, 1 + 2 * (y % 2))

    def p_b(k):
        await_scales(k)
        pg(k).wait_recv()

        def take(cols, r):
            acc[(k + 1) % NZ, :, cols] = r

        expert(k, pair_sources, w, y % 2, take)

    def p_c(k):
        def take(cols, r):
            o[k, 0:2, :, cols] = (acc[(k + 1) % NZ, :, cols] + r).astype(BF).reshape(2, ROWS, 256)

        expert(k, pair_sources, w2, 1 - y % 2, take)
        pr(k).start()

    def p_e(k):
        pr(k).wait_recv()
        zsum[k] = (o[k, 0].astype(F32) + f[k, 0].astype(F32)).astype(BF)
        pl.when(k > 0)(lambda: zb(k).start())

    def t_d(s):
        arrived(h.at[s], h_r.at[s - 3])
        o[s, 1, 0:HALF] = (o[s, 1, 0:HALF].astype(F32) + h[s, 0].astype(F32)).astype(BF)
        rs(s, 2).start()
        o[s, 3, HALF:ROWS] = (o[s, 3, HALF:ROWS].astype(F32) + h[s, 1].astype(F32)).astype(BF)
        rs(s, 3).start()

    def t_e(s):
        arrived(f.at[s], f_r.at[s - 3])
        zsum[s] = (
            o[s, 0].astype(F32) + f[s, 0].astype(F32) + f[s, 1].astype(F32)
        ).astype(BF)
        zb(s).start()

    loads = [
        pltpu.make_async_copy(src, dst, load_sem.at[k])
        for k, (src, dst) in enumerate(
            (
                (gain_hbm, gain_in),
                (gate_in, masters.at[0]),
                (up_in, masters.at[1]),
                (down_in, masters.at[2]),
                (tokens_in, tok),
                (group_hbm, group_in),
                (fine_hbm, fine_in),
                (route_hbm, route_in),
            )
        )
    ]
    for load in loads:
        load.start()
    barrier = pltpu.get_barrier_semaphore()
    peers = [{"x": (x + k) % NX} for k in range(1, NX)] + [{"c": 1 - c}]
    for peer in peers:
        pl.semaphore_signal(barrier, inc=1, device_id=peer, device_id_type=MESH)

    def greet(q, carry):
        peer = {"z": (z + q // NY) % NZ, "y": (y + q % NY) % NY}
        pl.semaphore_signal(barrier, inc=1, device_id=peer, device_id_type=MESH)
        return carry

    lax.fori_loop(1, NZ * NY, greet, 0)

    pair = remote(pieces.at[1 - c], other, sem_of("pair"), pair_r, {"c": 1 - c})

    for load in loads[:4]:
        load.wait()
    eye = lax.broadcasted_iota(jnp.int32, (64, 64), 0) == lax.broadcasted_iota(
        jnp.int32, (64, 64), 1
    )
    gain = jnp.sum(jnp.where(eye, gain_in[...], 0.0), axis=1, keepdims=True)

    def cast(e, carry):
        for m in range(3):
            value = masters[m, e] if m == 2 else gain * masters[m, e]
            value = value.astype(BF)
            pieces[0, e, m] = value[:32]
            pieces[1, e, m] = value[32:]
        return carry

    with jax.named_scope("cast"):
        lax.fori_loop(0, NZ * FINE, cast, 0, unroll=4)
    with jax.named_scope("barrier"):
        pl.semaphore_wait(barrier, NZ * NY - 1 + len(peers))
    pair.start()

    for load in loads[4:]:
        load.wait()

    def norm(r, carry):
        wide = tok[pl.ds(pl.multiple_of(r * ROWS, ROWS), ROWS), :].astype(F32)
        mean = jnp.sum(wide * wide, axis=1, keepdims=True) * (1.0 / D)
        normed[pl.ds(pl.multiple_of(r * ROWS, ROWS), ROWS), :] = (
            wide * lax.rsqrt(mean + EPS)
        ).astype(BF)
        return carry

    with jax.named_scope("norm"):
        lax.fori_loop(0, NZ, norm, 0)
        count = NZ * ROWS
        placing = placing_of(group_in[...])
        entry = lax.broadcasted_iota(jnp.int32, (8, count), 0)
        fine_id = entry % FINE
        weight = jnp.where(fine_in[0:1] == fine_id, route_in[0:1], 0.0) + jnp.where(
            fine_in[1:2] == fine_id, route_in[1:2], 0.0
        )
        top = weight.astype(BF).astype(F32)
        weight = jnp.where(entry < FINE, top, weight - top)
        weight = jnp.concatenate([weight, jnp.zeros((8, count), F32)], axis=0).astype(BF)
        sorted_weight = lax.dot_general(
            weight, placing, (((1,), (1,)), ((), ())), preferred_element_type=F32
        )
        sorted_weight = sorted_weight[0:FINE] + sorted_weight[FINE : 2 * FINE]
        for e in range(FINE):
            for p in range(2):
                scales[p, e // 2, e % 2] = sorted_weight[e : e + 1, LANE * p : LANE * p + LANE]
        for nb in range(8):
            part = jnp.dot(
                placing, normed[:, 256 * nb : 256 * nb + 256], preferred_element_type=F32
            )
            rows_in[:, :, 256 * nb : 256 * nb + 256] = part.astype(BF).reshape(NZ, ROWS, 256)

    with jax.named_scope("pair"):
        pair.wait_recv()

    def join(s):
        for n in range(FINE):
            e = FINE * to_z(s) + n
            mine, theirs = pieces[c, e], other[e]
            low = jnp.where(c == 0, mine, theirs)
            high = jnp.where(c == 0, theirs, mine)
            wsend[e] = jnp.concatenate([low, high], axis=-1)

    def send(copy, first, last):
        def one(s, carry):
            copy(s)
            return carry

        lax.fori_loop(first, last, one, 0)

    def send_w(s):
        join(s)
        for k in (1, 3, 2, 0):
            ws(s, k).start()

    def send_t(k):
        zt(k).start()
        for j in range(NY):
            wt(k, j).start()

    join(0)
    for k in (1, 3, 2):
        ws(0, k, "ws0").start()
    w[:, x, NY * z + y, c] = wsend[FINE * z + y]
    send(send_w, 1, 3)
    send(send_t, 1, 3)
    p_a(0)
    send(send_w, 3, NZ)
    send(send_t, 3, NZ)
    for j in range(1, NY):
        wt(0, j, "wt0").start()
    near[0, 0] = scales[z // 4, y // 2]
    a[0, 0] = rows_in[z]

    def run(fn, s):
        with jax.named_scope(fn.__name__):
            fn(s)

    def at(i, when, *todo):
        @pl.when(i == when)
        def _():
            for fn, s in todo:
                run(fn, s)

    run(w_b, 0)
    run(w_b, 1)
    run(p_a, 1)
    run(p_a, 2)

    def w_loop(i, carry):
        pl.when(i < NZ - 2)(lambda: run(w_b, i + 2))
        pl.when(i < NZ)(lambda: run(w_c, i))
        pl.when(i >= 2)(lambda: run(w_d, i - 2))
        at(i, 5, (t_a, 3), (t_a, 4))
        at(i, 6, (v_b, 0))
        at(i, 7, (v_b, 1), (t_b, 3))
        at(i, 8, (v_b, 2), (v_b, 3), (t_b, 4))
        at(i, 9, (v_b, 4), (t_a, 5), (t_a, 6))
        return carry

    lax.fori_loop(0, NZ + 2, w_loop, 0)

    with jax.named_scope("w_end"):
        arrived(w.at[:, :, :, 0], cw_r)
    def v_start(s, carry):
        v_b(s)
        return carry

    def t_loop(i, carry):
        at(i, 1, (v_c, 1), (p_b, 1), (t_b, 5), (v_c, 2))
        run(t_c, i + 3)

        @pl.when(i == 0)
        def _():
            lax.fori_loop(5, NZ, v_start, 0)

        at(i, 0, (v_c, 0))
        at(i, 1, (t_b, 6), (t_d, 3), (v_c, 3))
        at(i, 2, (t_d, 4), (v_c, 4))
        at(i, 3, (v_c, 6), (t_e, 3))
        pl.when(i >= 2)(lambda: run(p_b, (4 - 2 * (i - 1)) % 4))
        at(i, 2, (v_c, 5))
        at(i, 3, (v_c, 7), (t_d, 5), (v_d, 0), (v_d, 1), (t_d, 6), (p_a, 7), (t_e, 4))
        at(i, 3, *((v_d, k) for k in range(2, NZ)))
        at(i, 3, (t_e, 5))
        return carry

    lax.fori_loop(0, NZ - PAIRED, t_loop, 0)
    with jax.named_scope("v_end"):
        arrived(w2.at[:, :, :, 0], cv_r)

    def p_at(i):
        return (i + 1) % 4 + 4 * ((i // 2) * (3 - i))

    def p_loop(i, carry):
        run(p_c, p_at(i))
        at(i, 0, (t_e, 6))
        at(i, 1, (p_b, 7))
        return carry

    lax.fori_loop(0, PAIRED, p_loop, 0)

    def e_loop(i, carry):
        run(p_e, p_at(i))
        return carry

    lax.fori_loop(0, PAIRED, e_loop, 0)
    back[z] = zsum[0]
    many = NZ - 1
    all_sent(pieces.at[0], "pair")
    all_sent(rows_in.at[pl.ds(0, many)], "zt")
    all_sent(near.at[0, pl.ds(0, NY - 1)], "wt0")
    all_sent(near.at[pl.ds(0, many)], "wt")
    all_sent(wsend.at[pl.ds(0, NY - 1)], "ws0")
    all_sent(wsend.at[pl.ds(0, many * NY)], "ws")
    all_sent(wsend, "sw")
    all_sent(w.at[:, pl.ds(0, 3), :, 0], "xw")
    all_sent(w2.at[:, pl.ds(0, 3), :, 0], "xv")
    all_sent(w.at[:, :, :, 0], "cw")
    all_sent(w2.at[:, :, :, 0], "cv")
    all_sent(a.at[pl.ds(0, NZ - PAIRED), pl.ds(0, 3)], "ag")
    all_sent(o.at[pl.ds(0, NZ - PAIRED), pl.ds(0, 3)], "rs")
    all_sent(a.at[pl.ds(0, PAIRED), 0], "pg")
    all_sent(o.at[pl.ds(0, PAIRED), 0], "pr")
    with jax.named_scope("finish"):
        arrived(back.at[pl.ds(0, many)], zb_r)
    all_sent(back.at[pl.ds(0, many)], "zb")


def settle(back, w, group_in, mixed_out, g_out, u_out, d_out, mixed, out_sem, mixed_sem):
    outs = (g_out, u_out, d_out)
    writes = [
        pltpu.make_async_copy(
            w.at[m, xb], outs[m].at[:, :, :, pl.ds(LANE * xb, LANE)], out_sem.at[m, xb]
        )
        for m in range(3)
        for xb in range(NX)
    ]
    for write in writes:
        write.start()
    placing = placing_of(group_in[...])
    lasts = []
    for nb in range(4):
        cols = pl.ds(512 * nb, 512)
        mixed[:, cols] = lax.dot_general(
            placing, back[:, cols], (((0,), (0,)), ((), ())), preferred_element_type=F32
        ).astype(BF)
        last = pltpu.make_async_copy(mixed.at[:, cols], mixed_out.at[:, cols], mixed_sem.at[nb])
        last.start()
        lasts.append(last)
    for copy in writes + lasts:
        copy.wait()


def exchange(tokens, group, fine, route, gain, gate, up, down):
    hbm = pl.BlockSpec(memory_space=pltpu.HBM)
    vmem = pl.BlockSpec(memory_space=pltpu.VMEM)
    ready = jax.ShapeDtypeStruct((32, 2, 32, 512), BF)
    dma = pltpu.SemaphoreType.DMA
    count = NZ * ROWS
    scratch = [
        pltpu.VMEM((1, count), jnp.int32),
        pltpu.VMEM((2, count), jnp.int32),
        pltpu.VMEM((2, count), F32),
        pltpu.VMEM((1, 64), F32),
        pltpu.VMEM((count, D), BF),
        pltpu.VMEM((3, 32, 64, 64), F32),
        pltpu.VMEM((count, D), BF),
        pltpu.VMEM((NZ, ROWS, D), BF),
        pltpu.VMEM((2, 32, 3, 32, 64), BF),
        pltpu.VMEM((2, 2, 2, 1, LANE), F32),
        pltpu.VMEM((NZ, NY, 2, 1, LANE), F32),
        pltpu.VMEM((NZ, NY, ROWS, D), BF),
        pltpu.VMEM((NZ, NY, ROWS, D), BF),
        pltpu.VMEM((NZ, 2, HALF, D), BF),
        pltpu.VMEM((NZ, 2, ROWS, D), BF),
        pltpu.VMEM((NZ, ROWS, D), BF),
        pltpu.VMEM((32, 3, 32, LANE), BF),
        pltpu.VMEM((32, 3, 32, 64), BF),
        pltpu.VMEM((3, NX, 32, 2, 32, LANE), BF),
        pltpu.VMEM((PAIRED, 2 * ROWS, D), F32),
        dma((8,)), dma((len(SENT),)),
        dma, dma, dma, dma,
        dma((NZ,)), dma((NZ,)), dma((NZ,)), dma((NZ,)),
        dma((PAIRED,)), dma((PAIRED,)),
        dma((NZ - PAIRED,)), dma((NZ - PAIRED,)),
        dma((NZ - PAIRED, 3)), dma((NZ, 3)), dma((NZ, 3)),
    ]
    back, w = pl.pallas_call(
        kernel,
        out_shape=(
            pltpu.VMEM((NZ, ROWS, D), BF),
            pltpu.VMEM((3, NX, 32, 2, 32, LANE), BF),
        ),
        in_specs=[hbm] * 8,
        out_specs=(vmem, vmem),
        scratch_shapes=scratch,
        compiler_params=pltpu.CompilerParams(
            collective_id=0, has_side_effects=True, vmem_limit_bytes=56 * 1024 * 1024
        ),
    )(tokens, group, fine, route, gain, gate, up, down)
    return pl.pallas_call(
        settle,
        out_shape=(jax.ShapeDtypeStruct((count, D), BF), ready, ready, ready),
        in_specs=[vmem, vmem, vmem],
        out_specs=(hbm,) * 4,
        scratch_shapes=[pltpu.VMEM((count, D), BF), dma((3, NX)), dma((4,))],
        compiler_params=pltpu.CompilerParams(vmem_limit_bytes=16 * 1024 * 1024),
    )(back.reshape(count, D), w, group)


def local(
    tokens, expert_group, expert_fine, route_weight, norm_gain, gate_master, up_master, down_master
):
    mixed, gate, up, down = exchange(
        tokens,
        expert_group.reshape(1, -1),
        expert_fine.T,
        route_weight.T,
        norm_gain.reshape(1, -1),
        gate_master,
        up_master,
        down_master,
    )
    return (mixed,) + tuple(r.reshape(1, D, 512) for r in (gate, up, down))


def solution(mesh):
    fine = Mesh(mesh.devices.reshape(NZ, NY, NX, 2), ("z", "y", "x", "c"))
    fs, tp = ("z", "y"), ("x", "c")
    token = fs + tp
    in_specs = (
        P(token, None),
        P(token),
        P(token, None),
        P(token, None),
        P(fs),
        P(None, fs, tp),
        P(None, fs, tp),
        P(None, fs, tp),
    )
    out_specs = (
        P(token, None),
        P(fs, None, None),
        P(fs, None, None),
        P(fs, None, None),
    )
    return jax.shard_map(local, mesh=fine, in_specs=in_specs, out_specs=out_specs, check_vma=False)
```
